128 devices in a mesh: ep: 128 (over z, y, x, core).
Axes of the slice: x: 4, y: 4, z: 4, core: 2. Of those that a mesh axis runs over, the one named last changes fastest.
Arguments:
- tokens: bfloat16 [512, 2048], P('ep'), may hold values from -6 to 6
- recurrent_state: float32 [512, 8, 128, 128], P('ep'), may hold values from -4 to 4
- query_weight: bfloat16 [2048, 1024], P(None, 'ep'), may hold values from -0.125 to 0.125
- forget_weight: bfloat16 [2048, 1024], P(None, 'ep'), may hold values from -0.125 to 0.125
- input_weight: bfloat16 [2048, 1024], P(None, 'ep'), may hold values from -0.125 to 0.125
- outgate_weight: bfloat16 [2048, 1024], P(None, 'ep'), may hold values from -0.125 to 0.125
- lower_bound: float32 [1024], replicated, may hold values from 0 to 0.9
- head_gain: float32 [128], replicated, may hold values from 0.1 to 1.9
- mixout_weight: bfloat16 [1024, 2048], P(None, 'ep'), may hold values from -0.1875 to 0.1875
- first_gain: float32 [2048], replicated, may hold values from 0.1 to 1.9
- first_bias: float32 [2048], replicated, may hold values from -1.5 to 1.5
- router_weight: bfloat16 [2048, 8], replicated, may hold values from -0.125 to 0.125
- branch_vector: bfloat16 [2048], replicated, may hold values from -0.125 to 0.125
- dense_gate_weight: bfloat16 [2048, 5632], P(None, 'ep'), may hold values from -0.125 to 0.125
- dense_up_weight: bfloat16 [2048, 5632], P(None, 'ep'), may hold values from -0.125 to 0.125
- dense_down_weight: bfloat16 [5632, 2048], P('ep'), may hold values from -0.078125 to 0.078125
- expert_gate_weight: bfloat16 [2048, 57344], P(None, 'ep'), may hold values from -0.125 to 0.125
- expert_up_weight: bfloat16 [2048, 57344], P(None, 'ep'), may hold values from -0.125 to 0.125
- expert_down_weight: bfloat16 [57344, 2048], P('ep'), may hold values from -0.0625 to 0.0625
- second_gain: float32 [2048], replicated, may hold values from 0.1 to 1.9
- second_bias: float32 [2048], replicated, may hold values from -1.5 to 1.5
- routes: int32 [512, 2], replicated, may hold values from 0 to 7, all different within a row; in each aligned block of 4 rows (0 to 3, 4 to 7, ...) at most 2 rows name the same one
Outputs:
- output: bfloat16 [512, 2048], P('ep')
- new_state: float32 [512, 8, 128, 128], P('ep')
The draws below stay inside these ranges and needn't reach their ends.
Inputs may be any that keep to these rules, and one draw needn't show every extreme that they name: `routes`: each row names two different experts; in the rows of one device no expert is named more than 2 times, a bound that some block reaches in some device's rows.
All inputs are finite; a program needn't handle non-finite values.
Results may differ from the reference program's by a relative error of at most 0.0095.
Values may be sent and summed in bfloat16 or wider, within the bound.
A program may use at most 64 MiB of HBM per device.

```python
import math
import jax
import jax.numpy as jnp
import numpy as np
from jax import lax

D = 2048
HGW = 1024
DK = 128
HEADS = 8
EXPERTS = 8
FF_E = 7168
FD = 5632
B_DEV = 4
CAP = 2
TOKENS = 512
N_EP = 128


def block_scale(rng, extent, cuts, least, high):
    level, own = 1.0, jax.random.fold_in(rng, 6)
    for axis_at, blocks in cuts:
        draws = jnp.exp(jax.random.uniform(jax.random.fold_in(own, axis_at), (blocks,), jnp.float32, least / len(cuts), high / len(cuts)))
        level = level * jnp.repeat(draws, extent[axis_at] // blocks).reshape([-1 if axis == axis_at else 1 for axis in range(len(extent))])
    return level


def deal_out(key, own, number, rows, amount, top, reach, skew):
    order = jax.random.permutation(key, amount)
    crowded, usual = portions_of(amount, rows * top, reach, skew, True), portions_of(amount, rows * top, reach, skew, False)
    places = jnp.arange(amount)

    def named(sizes, rotation):
        used = int((sizes > 0).sum())
        fixed = max(1, used // 4)
        moved = fixed + (places - fixed + rotation * (used - fixed)) % max(1, amount - fixed)
        return jnp.zeros((amount,), jnp.int32).at[order[jnp.where(places < fixed, places, moved)]].set(jnp.asarray(sizes, jnp.int32))

    sizes = jnp.where(number % 4 == 0, named(crowded, number // 4), named(usual, number - number // 4 - 1))
    mixed = jax.random.permutation(jax.random.fold_in(own, 3), amount)
    donor, sink = mixed[0:amount // 2 * 2:2], mixed[1:amount // 2 * 2:2]
    room = jnp.minimum(sizes[donor] - 1, reach - sizes[sink]) // 2
    room = jnp.where((donor == order[0]) | (sink == order[0]) | (sizes[sink] == 0), 0, jnp.maximum(room, 0))
    moved = jax.random.randint(jax.random.fold_in(own, 4), (amount // 2,), 0, 1 << 20) % (room + 1)
    sizes = sizes.at[donor].add(-moved).at[sink].add(moved)
    members = jnp.searchsorted(jnp.cumsum(sizes), jnp.arange(rows * top), side="right").astype(jnp.int32)
    table = members.reshape(top, rows).T
    table = table[jax.random.permutation(jax.random.fold_in(own, 1), rows)]
    rotation = jax.random.randint(jax.random.fold_in(own, 2), (rows, 1), 0, top)
    return jnp.take_along_axis(table, (jnp.arange(top)[None, :] + rotation) % top, axis=1)


def portions_of(amount, total, reach, slope, full):
    weights = [(1 << 20) // math.isqrt(rank ** slope) + 1 for rank in range(1, amount + 1)]
    largest = reach if full else min(reach, max(-(-total // amount), total * weights[0] // sum(weights)))
    least = 1 if total - largest >= amount - 1 else 0
    holding, spare = [largest] + [least] * (amount - 1), total - largest - least * (amount - 1)
    while spare > 0:
        free = [i for i in range(1, amount) if holding[i] < largest] or [i for i in range(1, amount) if holding[i] < reach]
        mass, remaining = sum([weights[i] for i in free]), spare
        for i in free:
            addition = min(reach - holding[i], max(1, remaining * weights[i] // mass), spare)
            holding[i] = holding[i] + addition
            spare = spare - addition
    return np.array(holding)


def bell_draw(stream_key, shape, scale, limit, pieces=(), kind=jnp.bfloat16):
    level = block_scale(stream_key, shape, pieces, -0.22, 0.18) if pieces else 1.0
    result = jax.random.normal(stream_key, shape, jnp.float32) * scale * level
    return jnp.minimum(jnp.maximum(result, -limit), limit).astype(kind)


def setup_inputs(seed: int = 0) -> dict:
    keys = jax.random.split(jax.random.key(seed), 23)
    tokens = bell_draw(keys[0], (TOKENS, D), 1.0, 6.0, ((0, 128),))
    recurrent_state = bell_draw(keys[1], (TOKENS, HEADS, DK, DK), 0.5, 4.0, ((0, 128),), jnp.float32)
    query_weight = bell_draw(keys[2], (D, HGW), D ** -0.5, 0.125, ((1, 128),))
    forget_weight = bell_draw(keys[3], (D, HGW), D ** -0.5, 0.125, ((1, 128),))
    input_weight = bell_draw(keys[4], (D, HGW), D ** -0.5, 0.125, ((1, 128),))
    outgate_weight = bell_draw(keys[5], (D, HGW), D ** -0.5, 0.125, ((1, 128),))
    lower_bound = jnp.clip(jax.random.uniform(keys[6], (HGW,), jnp.float32, 0.0, 0.9), 0.0, 0.9)
    head_gain = jnp.clip(1.0 + 0.18 * jax.random.normal(keys[7], (DK,), jnp.float32), 0.1, 1.9)
    mixout_weight = bell_draw(keys[8], (HGW, D), HGW ** -0.5, 0.1875, ((1, 128),))
    first_gain = jnp.clip(1.0 + 0.18 * jax.random.normal(keys[9], (D,), jnp.float32), 0.1, 1.9)
    first_bias = bell_draw(keys[10], (D,), 0.3, 1.5, (), jnp.float32)
    router_weight = bell_draw(keys[11], (D, EXPERTS), D ** -0.5, 0.125)
    branch_vector = bell_draw(keys[12], (D,), D ** -0.5, 0.125)
    dense_gate_weight = bell_draw(keys[13], (D, FD), D ** -0.5, 0.125, ((1, 128),))
    dense_up_weight = bell_draw(keys[14], (D, FD), D ** -0.5, 0.125, ((1, 128),))
    dense_down_weight = bell_draw(keys[15], (FD, D), FD ** -0.5, 0.078125, ((0, 128),))
    expert_gate_weight = bell_draw(keys[16], (D, EXPERTS * FF_E), D ** -0.5, 0.125, ((1, 128),))
    expert_up_weight = bell_draw(keys[17], (D, EXPERTS * FF_E), D ** -0.5, 0.125, ((1, 128),))
    expert_down_weight = bell_draw(keys[18], (EXPERTS * FF_E, D), FF_E ** -0.5, 0.0625, ((0, 128),))
    second_gain = jnp.clip(1.0 + 0.18 * jax.random.normal(keys[19], (D,), jnp.float32), 0.1, 1.9)
    second_bias = bell_draw(keys[20], (D,), 0.3, 1.5, (), jnp.float32)
    routes_keys = jax.random.split(jax.random.fold_in(keys[21], 1), TOKENS // B_DEV)
    routes_turns = jax.random.permutation(jax.random.fold_in(keys[21], 3), TOKENS // B_DEV)
    routes = jax.vmap(lambda own, number: deal_out(jax.random.fold_in(keys[21], 2), own, number, B_DEV, EXPERTS, 2, CAP, 2))(routes_keys, routes_turns).reshape((TOKENS, 2))
    return dict(tokens=tokens, recurrent_state=recurrent_state, query_weight=query_weight, forget_weight=forget_weight, input_weight=input_weight, outgate_weight=outgate_weight, lower_bound=lower_bound, head_gain=head_gain, mixout_weight=mixout_weight, first_gain=first_gain, first_bias=first_bias, router_weight=router_weight, branch_vector=branch_vector, dense_gate_weight=dense_gate_weight, dense_up_weight=dense_up_weight, dense_down_weight=dense_down_weight, expert_gate_weight=expert_gate_weight, expert_up_weight=expert_up_weight, expert_down_weight=expert_down_weight, second_gain=second_gain, second_bias=second_bias, routes=routes)


ALPHA = 8.0 ** 0.25
NORM_EPS = 1e-05
HEAD_EPS = 1e-06

def layer_norm(mixture, gain, bias):
    center = lax.optimization_barrier(jnp.mean(mixture, axis=-1, keepdims=True))
    spread = lax.optimization_barrier(jnp.mean(jnp.square(mixture - center), axis=-1, keepdims=True))
    return (mixture - center) * lax.rsqrt(spread + NORM_EPS) * gain + bias

def recurrence(projected, state, lower_bound, head_gain):
    nseq, heads, width = (state.shape[0], state.shape[1], state.shape[2])
    query = projected[:, 0].astype(jnp.float32).reshape(nseq, heads, width)
    forget_in = projected[:, 1].astype(jnp.float32)
    value = projected[:, 2].astype(jnp.float32).reshape(nseq, heads, width)
    outgate = projected[:, 3].astype(jnp.float32)
    forget = (lower_bound + (1.0 - lower_bound) * jax.nn.sigmoid(forget_in)).reshape(nseq, heads, width)
    keyed = ((1.0 - lower_bound) * jax.nn.sigmoid(-forget_in)).reshape(nseq, heads, width)
    fresh = forget[..., None] * state + keyed[..., None] * value[:, :, None, :]
    read = jnp.einsum('bhkv,bhk->bhv', fresh, query, precision=lax.Precision.HIGHEST)
    scaled = read * lax.rsqrt(lax.optimization_barrier(jnp.mean(jnp.square(read), axis=-1, keepdims=True)) + HEAD_EPS) * head_gain
    mixed = (scaled.reshape(nseq, heads * width) * jax.nn.silu(outgate)).astype(jnp.bfloat16)
    return (mixed, fresh)

def reference(tokens, recurrent_state, query_weight, forget_weight, input_weight, outgate_weight, lower_bound, head_gain, mixout_weight, first_gain, first_bias, router_weight, branch_vector, dense_gate_weight, dense_up_weight, dense_down_weight, expert_gate_weight, expert_up_weight, expert_down_weight, second_gain, second_bias, routes):
    f32 = jnp.float32
    parts = [jnp.dot(tokens, weight, preferred_element_type=f32).astype(jnp.bfloat16) for weight in (query_weight, forget_weight, input_weight, outgate_weight)]
    projected = jnp.stack(parts, axis=1)
    mixed, new_state = recurrence(projected, recurrent_state, lower_bound, head_gain)
    mix_out = jnp.dot(mixed, mixout_weight, preferred_element_type=f32).astype(jnp.bfloat16)
    normed = layer_norm(ALPHA * tokens.astype(f32) + mix_out.astype(f32), first_gain, first_bias).astype(jnp.bfloat16)
    width = normed.shape[1]
    logits = jnp.dot(normed, router_weight, preferred_element_type=f32)
    expert_ids = jnp.arange(EXPERTS, dtype=jnp.int32)
    first_pick = routes[:, 0]
    second_pick = routes[:, 1]
    first_logit = lax.optimization_barrier(jnp.sum(jnp.where(first_pick[:, None] == expert_ids[None, :], logits, 0.0), axis=1))
    second_logit = lax.optimization_barrier(jnp.sum(jnp.where(second_pick[:, None] == expert_ids[None, :], logits, 0.0), axis=1))
    share = jax.nn.sigmoid(first_logit - second_logit)
    branch_gate = jax.nn.sigmoid(jnp.dot(normed, branch_vector, preferred_element_type=f32))
    dense_hidden = (jax.nn.silu(jnp.dot(normed, dense_gate_weight, preferred_element_type=f32)) * jnp.dot(normed, dense_up_weight, preferred_element_type=f32)).astype(jnp.bfloat16)
    channel = branch_gate[:, None] * jnp.dot(dense_hidden, dense_down_weight, preferred_element_type=f32)
    blocks = normed.reshape(N_EP, B_DEV, width).astype(f32)
    slot_ids = jnp.arange(CAP, dtype=jnp.int32)
    for expert in range(EXPERTS):
        on_first = first_pick == expert
        on_second = second_pick == expert
        token_weight = share * on_first.astype(f32) + (1.0 - share) * on_second.astype(f32)
        hits = (on_first | on_second).astype(jnp.int32).reshape(N_EP, B_DEV)
        ranks = jnp.cumsum(hits, axis=1) - 1
        select = ((ranks[:, None, :] == slot_ids[None, :, None]) & (hits[:, None, :] > 0)).astype(f32)
        slot_rows = jnp.einsum('sci,sid->scd', select, blocks, precision=lax.Precision.HIGHEST)
        slot_rows = slot_rows.astype(jnp.bfloat16).reshape(N_EP * CAP, width)
        low = expert * FF_E
        gate_part = jnp.dot(slot_rows, expert_gate_weight[:, low:low + FF_E], preferred_element_type=f32)
        up_part = jnp.dot(slot_rows, expert_up_weight[:, low:low + FF_E], preferred_element_type=f32)
        hidden = (jax.nn.silu(gate_part) * up_part).astype(jnp.bfloat16)
        slot_out = jnp.dot(hidden, expert_down_weight[low:low + FF_E, :], preferred_element_type=f32)
        slot_out = slot_out.reshape(N_EP, CAP, width)
        back = jnp.einsum('sci,scd->sid', select, slot_out, precision=lax.Precision.HIGHEST)
        channel = channel + back.reshape(N_EP * B_DEV, width) * token_weight[:, None]
    output = layer_norm(ALPHA * normed.astype(f32) + channel, second_gain, second_bias).astype(jnp.bfloat16)
    return (output, new_state)
```

```python
import functools

import jax
import jax.numpy as jnp
from jax import lax
from jax.experimental import pallas as pl
from jax.experimental.pallas import tpu as pltpu
from jax.sharding import PartitionSpec as P

ALPHA = 8.0**0.25
NORM_EPS = 1e-05
HEAD_EPS = 1e-06
HALF = 1024
F32 = jnp.float32
BF16 = jnp.bfloat16
PARTS = (
    (slice(0, 384), (2, 1, 0)),
    (slice(384, 768), (1, 0, 2)),
    (slice(768, 1024), (0, 2, 1)),
)
NT = (((1,), (1,)), ((), ()))


def dot(a, b):
    return jnp.dot(a, b, preferred_element_type=F32)


def dot_nt(a, b):
    return lax.dot_general(a, b, NT, preferred_element_type=F32)


def iota(shape, dim):
    return lax.broadcasted_iota(jnp.int32, shape, dim)


def sigmoid(a):
    return 1.0 / (1.0 + jnp.exp(-a))


def kernel(
    tok_h, state_h, wq_h, wf_h, wi_h, wo_h, lb_h, hg_h, wm_h, g1_h, b1_h, router_h, branch_h,
    dg_h, du_h, dd_h, eg_h, eu_h, ed_h, g2_h, b2_h, routes_h,
    out_ref, nst_h,
    tokv, st, nst, wp, lb, hg, wm, g1, b1, rt, br, dg, du, dd, eg, eu, ed, g2, b2, rts,
    tb, nb, msg, rcv, ob, xe, wd, wdd, rd,
    r1a, r1b, r1c, r2a, r2b, r2c, r3a, r3b, r3c, t1a, t1b, t1c, t2a, t2b, t2c,
    loc, stsem, nsem, pw_s, pw_r, wm_s, wm_r, wmx_s, wmx_r, tk_s, tk_r, nb_s, nb_r, a2_s, a2_r, rs_s, rs_r,
):
    me = lax.axis_index("ep")
    core = me % 2
    chip = me // 2
    at = (chip // 16, (chip // 4) % 4, chip % 4)
    partner = me + 1 - 2 * core

    def peer(dim, k):
        c = [at[0], at[1], at[2]]
        c[dim] = (c[dim] + k) % 4
        return 2 * ((c[0] * 4 + c[1]) * 4 + c[2]) + core

    def remote(src, dst, ss, rs, dev):
        pltpu.make_async_remote_copy(
            src_ref=src, dst_ref=dst, send_sem=ss, recv_sem=rs, device_id=(dev,),
            device_id_type=pl.DeviceIdType.MESH,
        ).start()

    def local(src, dst, sem):
        cp = pltpu.make_async_copy(src, dst, sem)
        cp.start()
        return cp

    def take(ref, sem):
        pltpu.make_async_copy(ref, ref, sem).wait()

    own = (at[0], at[1], at[2])
    c_tok = local(tok_h, tokv, loc.at[0])
    c_wp = [local(w, wp.at[i, core], loc.at[1 + i]) for i, w in enumerate((wq_h, wf_h, wi_h, wo_h))]
    c_wm = local(wm_h, wm.at[own + (core,)], loc.at[5])
    c_small = [
        local(a, b, loc.at[6 + i])
        for i, (a, b) in enumerate(
            ((lb_h, lb), (hg_h, hg), (g1_h, g1), (b1_h, b1), (router_h, rt), (branch_h, br),
             (g2_h, g2), (b2_h, b2), (routes_h, rts))
        )
    ]
    barrier = pltpu.get_barrier_semaphore()
    for dim in range(3):
        for k in range(1, 4):
            pl.semaphore_signal(barrier, inc=1, device_id=(peer(dim, k),), device_id_type=pl.DeviceIdType.MESH)
    pl.semaphore_signal(barrier, inc=1, device_id=(partner,), device_id_type=pl.DeviceIdType.MESH)
    c_tok.wait()
    toks = tokv[...].astype(F32)
    tblk = jnp.concatenate([toks[:, :HALF], toks[:, HALF:]], axis=0).astype(BF16)
    tb[own] = tblk
    pl.semaphore_wait(barrier, 10)

    def ag_send(buf, tail, part, phase, ss, rs):
        lanes, order = PARTS[part]
        idx = tuple(slice(None) if d in order[:phase] else at[d] for d in range(3))
        ref = buf.at[idx + tail + (slice(None), lanes)]
        for k in (2, 1, 3):
            remote(ref, ref, ss.at[part, phase], rs.at[part, phase], peer(order[phase], k))

    def three(buf, tail, part, phase):
        lanes, _ = PARTS[part]
        idx = ((0, 0, slice(0, 3)), (0, slice(0, 3), slice(None)), (slice(0, 3), slice(None), slice(None)))[phase]
        return buf.at[idx + tail + (slice(None), lanes)]

    def ag_take(buf, tail, part, phase, rs):
        take(three(buf, tail, part, phase), rs.at[part, phase])

    for part in range(3):
        ag_send(tb, (), part, 0, tk_s, tk_r)
    for i, w in enumerate((wq_h, wf_h, wi_h, wo_h)):
        remote(w, wp.at[i, core], pw_s.at[i], pw_r.at[i], partner)
    wtail = (core,)
    c_wm.wait()
    for part in range(3):
        ag_send(wm, wtail, part, 0, wm_s, wm_r)
    c_st = [local(state_h.at[t], st.at[t], stsem.at[t]) for t in range(4)]
    c_w = []
    for i, (a, b) in enumerate(((dg_h, dg), (du_h, du), (dd_h, dd), (eg_h, eg), (eu_h, eu), (ed_h, ed))):
        c_w.append(local(a, b.at[core], loc.at[15 + i]))
    for part in range(3):
        ag_take(tb, (), part, 0, tk_r)
        ag_send(tb, (), part, 1, tk_s, tk_r)
    for part in range(3):
        ag_take(wm, wtail, part, 0, wm_r)
        ag_send(wm, wtail, part, 1, wm_s, wm_r)
    for part in range(3):
        ag_take(tb, (), part, 1, tk_r)
        ag_send(tb, (), part, 2, tk_s, tk_r)
    for i, (a, b) in enumerate(((dg_h, dg), (du_h, du), (dd_h, dd), (eg_h, eg), (eu_h, eu), (ed_h, ed))):
        remote(a, b.at[core], pw_s.at[4 + i], pw_r.at[4 + i], partner)

    for c in c_small:
        c.wait()
    expert = chip // 8
    r0 = rts[0:1, :]
    r1 = rts[1:2, :]
    lane = iota((1, 512), 1)
    hit = jnp.where((r0 == expert) | (r1 == expert), 1.0, 0.0)
    other = jnp.where(r0 == expert, r1, r0).astype(F32)
    mine = (lane // 4) % 2 == core

    def own_rows(v):
        moved = jnp.where(core == 0, pltpu.roll(v, 4, 1), pltpu.roll(v, 508, 1))
        return jnp.where(mine, v, moved)

    hit = own_rows(hit)
    other = own_rows(other)
    rank = jnp.zeros_like(hit)
    for d in range(1, 4):
        rank = rank + jnp.where(lane % 4 >= d, pltpu.roll(hit, d, 1), 0.0)
    srow, slane = iota((128, 256), 0), iota((128, 256), 1)
    fits = (srow // 64 == (slane // 4) % 2) & ((srow % 64) // 2 == slane // 8)
    sels, spreads = [], []
    for u in range(2):
        cols = slice(256 * u, 256 * (u + 1))
        sel = jnp.where(
            fits & (rank[:, cols] == (srow % 2).astype(F32)), jnp.broadcast_to(hit[:, cols], (128, 256)), 0.0
        )
        sels.append(sel.astype(BF16))
        spreads.append(jnp.transpose(sel).astype(BF16))
    other_t = jnp.transpose(jnp.broadcast_to(other, (128, 512)))
    wl = iota((512, 128), 1)
    pick = jnp.where(wl == 96 + expert, 1.0, 0.0) - jnp.where(wl == 96 + other_t.astype(jnp.int32), 1.0, 0.0)
    e_row, e_col = iota((128, 512), 0), iota((128, 512), 1)
    spread_e = jnp.where((e_row // 16 == e_col // 128) & (e_row % 16 == e_col % 16), 1.0, 0.0).astype(BF16)
    m_row, m_col = iota((512, 512), 0), iota((512, 512), 1)
    in_place = (m_row // 8) % 8 == (m_col // 16) % 8
    s_row, s_col = iota((32, 512), 0), iota((32, 512), 1)
    fold = jnp.where((s_col // 64 == s_row % 8) & (s_col % 8 == s_row // 8), 1.0, 0.0).astype(BF16)

    for i in range(4):
        c_wp[i].wait()
        take(wp.at[i, 0], pw_r.at[i])
    w64 = wp.reshape(64, 2048)
    w128 = jnp.concatenate([w64[:, :HALF], w64[:, HALF:]], axis=0)
    for part in range(3):
        ag_take(wm, wtail, part, 1, wm_r)
    for part in range(3):
        ag_take(tb, (), part, 2, tk_r)
    for part in range(3):
        ag_send(wm, wtail, part, 2, wm_s, wm_r)
    proj = dot_nt(tb.reshape(512, HALF)[...], w128)
    proj = proj + pltpu.roll(pltpu.roll(proj, 508, 0), 64, 1)
    msg.reshape(512, 128)[...] = proj.astype(BF16)

    @pl.loop(1, 64)
    def _(j):
        to = (chip + j) % 64
        remote(msg.at[to], rcv.at[chip], a2_s, a2_r, 2 * to + core)

    rcv[chip] = msg[chip]

    wd[...] = jnp.zeros_like(wd)
    wdd[...] = jnp.zeros_like(wdd)
    for i in range(6):
        c_w[i].wait()
    for i, b in enumerate((dg, du, dd, eg, eu, ed)):
        take(b.at[0], pw_r.at[4 + i])
    for c in range(2):
        for h in range(2):
            ls = slice(HALF * h, HALF * (h + 1))
            wd[256 * h + 48 * c : 256 * h + 48 * c + 44, :] = dg[c, :, ls]
            wd[256 * h + 128 + 48 * c : 256 * h + 128 + 48 * c + 44, :] = du[c, :, ls]
            wdd[128 * h + 48 * c : 128 * h + 48 * c + 44, :] = dd[c, :, ls]
    for h in range(2):
        ls = slice(HALF * h, HALF * (h + 1))
        wd[256 * h + 96 : 256 * h + 104, :] = rt[:, ls]
        wd[256 * h + 104 : 256 * h + 105, :] = br[:, ls]

    take(rcv.at[0:63], a2_r)
    wide = dot(rcv.reshape(512, 128)[...], spread_e)
    wide = jnp.where(in_place, wide, 0.0).astype(BF16)
    rows = dot(fold, wide)
    query, f_in, value, outgate = (rows[:, 128 * i : 128 * (i + 1)] for i in range(4))
    low = jnp.concatenate([lb[...]] * 4, axis=0)
    forget = low + (1.0 - low) * sigmoid(f_in)
    keyed = (1.0 - low) * sigmoid(-f_in)
    cols = jnp.transpose(jnp.concatenate([forget, keyed, query, query], axis=0))
    c_out = []
    for t in range(4):
        c_st[t].wait()
        for h in range(8):
            r = 8 * t + h
            fresh = cols[:, r : r + 1] * st[t, h] + cols[:, 32 + r : 33 + r] * value[r : r + 1, :]
            nst[t, h] = fresh
            rd[r : r + 1, :] = jnp.sum(fresh * cols[:, 64 + r : 65 + r], axis=0, keepdims=True)
        c_out.append(local(nst.at[t], nst_h.at[t], nsem.at[t]))
    read = rd[...]
    scaled = read * lax.rsqrt(jnp.mean(read * read, axis=1, keepdims=True) + HEAD_EPS) * hg[...]
    mixed = (scaled * (outgate * sigmoid(outgate))).astype(BF16).astype(F32)
    spread_m = jnp.where(
        iota((32, HALF), 0) % 8 == iota((32, HALF), 1) // 128, jnp.concatenate([mixed] * 8, axis=1), 0.0
    ).astype(BF16)
    for part in range(3):
        ag_take(wm, wtail, part, 2, wm_r)
    remote(
        wm.at[:, :, :, core], wm.at[:, :, :, core], wmx_s, wmx_r, partner
    )
    take(wm.at[:, :, :, 0], wmx_r)
    mo = dot_nt(spread_m, wm.reshape(2048, HALF)[...])
    mo = jnp.sum(mo.reshape(4, 8, 2048), axis=1).astype(BF16).astype(F32)
    pre = ALPHA * toks + mo
    center = jnp.mean(pre, axis=1, keepdims=True)
    var = jnp.mean(jnp.square(pre - center), axis=1, keepdims=True)
    normed = ((pre - center) * lax.rsqrt(var + NORM_EPS) * g1[...] + b1[...]).astype(BF16).astype(F32)
    nblk = jnp.concatenate([normed[:, :HALF], normed[:, HALF:]], axis=0)
    nb[own] = nblk.astype(BF16)

    for phase in range(3):
        for part in range(3):
            if phase:
                ag_take(nb, (), part, phase - 1, nb_r)
            ag_send(nb, (), part, phase, nb_s, nb_r)
    for part in range(3):
        ag_take(nb, (), part, 2, nb_r)

    nbv = nb.reshape(512, HALF)
    for u in range(2):
        sel = dot(sels[u], nbv[256 * u : 256 * (u + 1), :]).astype(BF16)
        xe[64 * u : 64 * (u + 1), :HALF] = sel[:64]
        xe[64 * u : 64 * (u + 1), HALF:] = sel[64:]
    gate = dot_nt(xe[...], eg.reshape(896, 2048)[...])
    up = dot_nt(xe[...], eu.reshape(896, 2048)[...])
    hidden = (gate * sigmoid(gate) * up).astype(BF16)
    y2 = dot_nt(nbv[...], wd[...])
    first_half = (iota((512, 256), 0) // 4) % 2 == 0
    y = jnp.where(first_half, y2[:, :256], y2[:, 256:]).reshape(64, 8, 256)
    y = (y + pltpu.roll(y, 4, 1)).reshape(512, 256)
    yg = y[:, :128]
    weight = sigmoid(jnp.sum(yg * pick, axis=1, keepdims=True))
    branch = sigmoid(yg[:, 104:105])
    hd = yg * sigmoid(yg) * y[:, 128:] * branch
    top = (iota((512, 128), 0) // 4) % 2 == 0
    hdd = jnp.concatenate([jnp.where(top, hd, 0.0), jnp.where(top, 0.0, hd)], axis=1).astype(BF16)
    slots = dot(hidden, ed.reshape(896, 2048)[...]).astype(BF16)
    obv = ob.reshape(512, HALF)
    for u in range(2):
        ru = slice(256 * u, 256 * (u + 1))
        rows_u = jnp.concatenate([slots[64 * u : 64 * (u + 1), :HALF], slots[64 * u : 64 * (u + 1), HALF:]], axis=0)
        total = weight[ru] * dot(spreads[u], rows_u) + dot(hdd[ru], wdd[...])
        obv[ru, :] = total.astype(BF16)

    r1s, r2s, r3s = (r1a, r1b, r1c), (r2a, r2b, r2c), (r3a, r3b, r3c)
    t1s, t2s = (t1a, t1b, t1c), (t2a, t2b, t2c)

    def rs_send(src, axis, rank_of, dst, dim, part, phase):
        for k in (2, 1, 3):
            c = (at[dim] + k) % 4
            idx = [slice(None)] * rank_of
            idx[axis] = c
            remote(src.at[tuple(idx)], dst.at[k - 1], rs_s.at[part, phase], rs_r.at[part, phase], peer(dim, k))

    for part in range(3):
        lanes, order = PARTS[part]
        rs_send(ob.at[:, :, :, :, lanes], order[0], 3, r1s[part], order[0], part, 0)
    for part in range(3):
        lanes, order = PARTS[part]
        d1, d2, _ = order
        take(r1s[part], rs_r.at[part, 0])
        idx = tuple(at[d] if d == d1 else slice(None) for d in range(3))
        total = ob[idx + (slice(None), lanes)].astype(F32)
        for k in range(3):
            total = total + r1s[part][k].astype(F32)
        t1s[part][...] = total.astype(BF16)
        axis = [d for d in range(3) if d != d1].index(d2)
        rs_send(t1s[part], axis, 2, r2s[part], d2, part, 1)
    for part in range(3):
        d1, d2, d3 = PARTS[part][1]
        take(r2s[part], rs_r.at[part, 1])
        axis = [d for d in range(3) if d != d1].index(d2)
        idx = [slice(None)] * 2
        idx[axis] = at[d2]
        total = t1s[part][tuple(idx)].astype(F32)
        for k in range(3):
            total = total + r2s[part][k].astype(F32)
        t2s[part][...] = total.astype(BF16)
        rs_send(t2s[part], 0, 1, r3s[part], d3, part, 2)
    chans = []
    for part in range(3):
        d3 = PARTS[part][1][2]
        take(r3s[part], rs_r.at[part, 2])
        total = t2s[part][at[d3]].astype(F32)
        for k in range(3):
            total = total + r3s[part][k].astype(F32)
        chans.append(total)
    z = ALPHA * nblk + jnp.concatenate(chans, axis=1)

    def both(v):
        v = jnp.broadcast_to(v, (8, 128))
        return (v + pltpu.roll(v, 4, 0))[:, 0:1]

    def by_half(ref):
        v = ref[...]
        return jnp.concatenate(
            [jnp.broadcast_to(v[:, :HALF], (4, HALF)), jnp.broadcast_to(v[:, HALF:], (4, HALF))], axis=0
        )

    center = both(jnp.sum(z, axis=1, keepdims=True)) * (1.0 / 2048)
    dev = z - center
    var = both(jnp.sum(dev * dev, axis=1, keepdims=True)) * (1.0 / 2048)
    res = dev * lax.rsqrt(var + NORM_EPS) * by_half(g2) + by_half(b2)
    out_ref[:, :HALF] = res[:4].astype(BF16)
    out_ref[:, HALF:] = res[4:].astype(BF16)

    for c in c_out:
        c.wait()
    for i in range(4):
        take(wp.at[i, 0], pw_s.at[i])
    for i, b in enumerate((dg, du, dd, eg, eu, ed)):
        take(b.at[0], pw_s.at[4 + i])
    take(wm.at[:, :, :, 0], wmx_s)
    take(msg.at[0:63], a2_s)
    for part in range(3):
        for phase in range(3):
            take(three(tb, (), part, phase), tk_s.at[part, phase])
            take(three(nb, (), part, phase), nb_s.at[part, phase])
            take(three(wm, (0,), part, phase), wm_s.at[part, phase])
        take(r1s[part], rs_s.at[part, 0])
        take(r2s[part], rs_s.at[part, 1])
        take(r3s[part], rs_s.at[part, 2])


def per_device(
    tokens, recurrent_state, query_weight, forget_weight, input_weight, outgate_weight, lower_bound, head_gain,
    mixout_weight, first_gain, first_bias, router_weight, branch_vector, dense_gate_weight, dense_up_weight,
    dense_down_weight, expert_gate_weight, expert_up_weight, expert_down_weight, second_gain, second_bias, routes,
):
    args = (
        tokens, recurrent_state, query_weight.T, forget_weight.T, input_weight.T, outgate_weight.T,
        lower_bound.reshape(8, 128), head_gain.reshape(1, 128), mixout_weight.T, first_gain.reshape(1, 2048),
        first_bias.reshape(1, 2048), router_weight.T, branch_vector.reshape(1, 2048), dense_gate_weight.T,
        dense_up_weight.T, dense_down_weight, expert_gate_weight.T, expert_up_weight.T, expert_down_weight,
        second_gain.reshape(1, 2048), second_bias.reshape(1, 2048), routes.T,
    )
    lanes = [p[0].stop - p[0].start for p in PARTS]
    V = pltpu.VMEM
    sem = pltpu.SemaphoreType.DMA
    scratch = [
        V((4, 2048), BF16), V((4, 8, 128, 128), F32), V((4, 8, 128, 128), F32), V((4, 2, 8, 2048), BF16),
        V((8, 128), F32), V((1, 128), F32), V((4, 4, 4, 2, 16, HALF), BF16), V((1, 2048), F32), V((1, 2048), F32),
        V((8, 2048), BF16), V((1, 2048), BF16), V((2, 44, 2048), BF16), V((2, 44, 2048), BF16),
        V((2, 44, 2048), BF16), V((2, 448, 2048), BF16), V((2, 448, 2048), BF16), V((2, 448, 2048), BF16),
        V((1, 2048), F32), V((1, 2048), F32), V((2, 512), jnp.int32),
        V((4, 4, 4, 8, HALF), BF16), V((4, 4, 4, 8, HALF), BF16), V((64, 8, 128), BF16), V((64, 8, 128), BF16),
        V((4, 4, 4, 8, HALF), BF16), V((128, 2048), BF16), V((512, HALF), BF16), V((256, HALF), BF16),
        V((32, 128), F32),
        *[V((3, 4, 4, 8, n), BF16) for n in lanes], *[V((3, 4, 8, n), BF16) for n in lanes],
        *[V((3, 8, n), BF16) for n in lanes], *[V((4, 4, 8, n), BF16) for n in lanes],
        *[V((4, 8, n), BF16) for n in lanes],
        sem((21,)), sem((4,)), sem((4,)), sem((10,)), sem((10,)), sem((3, 3)), sem((3, 3)), sem(()), sem(()),
        sem((3, 3)), sem((3, 3)), sem((3, 3)), sem((3, 3)), sem(()), sem(()), sem((3, 3)), sem((3, 3)),
    ]
    hbm = pl.BlockSpec(memory_space=pl.ANY)
    return pl.pallas_call(
        kernel,
        out_shape=(jax.ShapeDtypeStruct((4, 2048), BF16), jax.ShapeDtypeStruct((4, 8, 128, 128), F32)),
        in_specs=[hbm] * 22,
        out_specs=(pl.BlockSpec(memory_space=pltpu.VMEM), hbm),
        scratch_shapes=scratch,
        compiler_params=pltpu.CompilerParams(
            collective_id=0, has_side_effects=True, vmem_limit_bytes=60 * 1024 * 1024
        ),
        name="layer",
    )(*args)


def solution(mesh):
    ep = "ep"
    cols, rows = P(None, ep), P(ep, None)
    return jax.shard_map(
        per_device,
        mesh=mesh,
        in_specs=(
            rows, P(ep, None, None, None), cols, cols, cols, cols, P(), P(), cols, P(), P(), P(), P(),
            cols, cols, rows, cols, cols, rows, P(), P(), P(),
        ),
        out_specs=(rows, P(ep, None, None, None)),
        check_vma=False,
    )
```

```python
import functools

import jax
import jax.numpy as jnp
from jax import lax
from jax.experimental import pallas as pl
from jax.experimental.pallas import tpu as pltpu
from jax.sharding import PartitionSpec as P

ALPHA = 8.0**0.25
NORM_EPS = 1e-05
HEAD_EPS = 1e-06
HALF = 1024
F32 = jnp.float32
BF16 = jnp.bfloat16
ALL = slice(None)
ORDERS = ((2, 1, 0), (1, 0, 2), (0, 2, 1))
LANES = (slice(0, 384), slice(384, 768), slice(768, 1024))
TAILS = tuple((ALL, lanes) for lanes in LANES)
WTAILS = ((ALL, slice(0, 8), slice(0, 384)), (ALL, slice(8, 16), slice(0, 384)), (ALL, ALL, slice(384, 512)))
NT = (((1,), (1,)), ((), ()))


def dot(a, b):
    return jnp.dot(a, b, preferred_element_type=F32)


def dot_nt(a, b):
    return lax.dot_general(a, b, NT, preferred_element_type=F32)


def iota(shape, dim):
    return lax.broadcasted_iota(jnp.int32, shape, dim)


def id_of(part):
    return part if isinstance(part, int) else id(part)


def sigmoid(a):
    return 1.0 / (1.0 + jnp.exp(-a))


def kernel(
    tok_h, state_h, wq_h, wf_h, wi_h, wo_h, lb_h, hg_h, wm_h, g1_h, b1_h, router_h, branch_h,
    dg_h, du_h, dd_h, eg_h, eu_h, ed_h, g2_h, b2_h, routes_h,
    out_h, nst_h,
    tokv, outv, st, nst, wp, lb, hg, wm, g1, b1, rt, br, dg, du, dd, eg, eu, ed, g2, b2, rts,
    tb, nb, msg, rcv, ob, xe, wd, wdd, rd,
    r1a, r1b, r1c, r2a, r2b, r2c, t1a, t1b, t1c, mx, mos, mor,
    loc, stsem, nsem, pw_s, pw_r, wm_s, wm_r, wmx_s, wmx_r, mx_s, mx_r, tk_s, tk_r, nb_s, nb_r, a2_s, a2_r, rs_s, rs_r,
):
    me = lax.axis_index("ep")
    core = me % 2
    chip = me // 2
    at = (chip // 16, (chip // 4) % 4, chip % 4)
    partner = me + 1 - 2 * core

    def peer(steps):
        c = [(at[d] + steps[d]) % 4 if steps.get(d) else at[d] for d in range(3)]
        return 2 * ((c[0] * 4 + c[1]) * 4 + c[2]) + core

    def remote(src, dst, ss, rs, dev):
        pltpu.make_async_remote_copy(
            src_ref=src, dst_ref=dst, send_sem=ss, recv_sem=rs, device_id=(dev,),
            device_id_type=pl.DeviceIdType.MESH,
        ).start()

    sent, due = {}, {}

    def local(src, dst, sem):
        cp = pltpu.make_async_copy(src, dst, sem)
        cp.start()
        return cp

    def expect(key, ref, ss, rs):
        key = tuple(map(id_of, key)) if isinstance(key, tuple) else id_of(key)
        sent[key] = functools.partial(take, ref, ss)
        due[key] = functools.partial(take, ref, rs)

    def got(key):
        key = tuple(map(id_of, key)) if isinstance(key, tuple) else id_of(key)
        due.pop(key)()

    def take(ref, sem):
        pltpu.make_async_copy(ref, ref, sem).wait()

    own = (at[0], at[1], at[2])
    c_tok = local(tok_h, tokv, loc.at[0])
    c_wp = [local(w, wp.at[i, core], loc.at[1 + i]) for i, w in enumerate((wq_h, wf_h, wi_h, wo_h))]
    half_own = pl.ds(pl.multiple_of(core * 512, 512), 512)
    c_wm = local(wm_h.at[:, half_own], wm.at[own + (core,)], loc.at[5])
    c_small = [
        local(a, b, loc.at[6 + i])
        for i, (a, b) in enumerate(
            ((lb_h, lb), (hg_h, hg), (g1_h, g1), (b1_h, b1), (router_h, rt), (branch_h, br),
             (g2_h, g2), (b2_h, b2), (routes_h, rts))
        )
    ]
    barrier = pltpu.get_barrier_semaphore()
    steps = [{d1: k1, d2: k2} for d1, d2 in ((0, 1), (0, 2), (1, 2)) for k1 in (2, 1, 3) for k2 in (2, 1, 3)]
    steps += [{d: k} for d in range(3) for k in (2, 1, 3)]
    for step in steps:
        pl.semaphore_signal(barrier, inc=1, device_id=(peer(step),), device_id_type=pl.DeviceIdType.MESH)
    pl.semaphore_signal(barrier, inc=1, device_id=(partner,), device_id_type=pl.DeviceIdType.MESH)
    c_tok.wait()
    toks = tokv[...].astype(F32)
    tblk = jnp.concatenate([toks[:, :HALF], toks[:, HALF:]], axis=0).astype(BF16)
    tb[own] = tblk
    pl.semaphore_wait(barrier, 37)

    def region(part, fixed):
        return tuple(fixed.get(d, ALL) for d in range(3))

    def blocks(buf, tail, count):
        idx = {3: (0, 0, slice(0, 3)), 4: (0, 0, ALL), 12: (0, slice(0, 3), ALL), 48: (slice(0, 3), ALL, ALL)}[count]
        return buf.at[idx + tail]

    def plane_send(buf, part, ss, rs):
        d1, d2, _ = ORDERS[part]
        ref = buf.at[own + TAILS[part]]
        for k2 in (2, 1, 3, 0):
            for k1 in (2, 1, 3, 0):
                if k1 or k2:
                    remote(ref, ref, ss.at[part, k2], rs.at[part, (4 - k2) % 4], peer({d1: k1, d2: k2}))
        for g in range(4):
            expect((ss, part, g), blocks(buf, TAILS[part], 4 if g else 3), ss.at[part, g], rs.at[part, g])

    def line_send(buf, part, g, ss, rs):
        d1, d2, d3 = ORDERS[part]
        got((ss, part, g))
        idx = region(part, {d2: (at[d2] + g) % 4, d3: at[d3]})
        ref = buf.at[idx + TAILS[part]]
        for k in (2, 1, 3):
            remote(ref, ref, ss.at[part, 4], rs.at[part, 4], peer({d3: k}))
        if g == 2:
            expect((ss, part, 4), blocks(buf, TAILS[part], 48), ss.at[part, 4], rs.at[part, 4])

    def walk_send(buf, part, phase, ss, rs):
        order = ORDERS[part]
        if phase:
            got((ss, part, phase - 1))
        idx = region(part, {d: at[d] for d in order[phase:]})
        ref = buf.at[idx + WTAILS[part]]
        for k in (2, 1, 3):
            remote(ref, ref, ss.at[part, phase], rs.at[part, phase], peer({order[phase]: k}))
        expect((ss, part, phase), blocks(buf, WTAILS[part], (3, 12, 48)[phase]), ss.at[part, phase], rs.at[part, phase])

    for part in range(3):
        plane_send(tb, part, tk_s, tk_r)
    half_in = pl.ds(pl.multiple_of((1 - core) * 512, 512), 512)
    remote(wm_h.at[:, half_in], wm.at[own + (core,)], wmx_s, wmx_r, partner)
    expect(wmx_s, wm.at[own + (0,)], wmx_s, wmx_r)
    for i, w in enumerate((wq_h, wf_h, wi_h, wo_h)):
        remote(w, wp.at[i, core], pw_s.at[i], pw_r.at[i], partner)
        expect((pw_s, i), wp.at[i, 0], pw_s.at[i], pw_r.at[i])
    c_st = [local(state_h.at[t], st.at[t], stsem.at[t]) for t in range(4)]
    c_w = []
    big = ((dg_h, dg), (du_h, du), (dd_h, dd), (eg_h, eg), (eu_h, eu), (ed_h, ed))
    for i, (a, b) in enumerate(big):
        c_w.append(local(a, b.at[core], loc.at[15 + i]))
    for g in (0, 1, 3, 2):
        for part in range(3):
            line_send(tb, part, g, tk_s, tk_r)
    c_wm.wait()
    got(wmx_s)
    for part in range(3):
        walk_send(wm, part, 0, wm_s, wm_r)
    for i, (a, b) in enumerate(big):
        remote(a, b.at[core], pw_s.at[4 + i], pw_r.at[4 + i], partner)
        expect((pw_s, 4 + i), b.at[0], pw_s.at[4 + i], pw_r.at[4 + i])

    for c in c_small:
        c.wait()
    expert = chip // 8
    r0 = rts[0:1, :]
    r1 = rts[1:2, :]
    lane = iota((1, 512), 1)
    hit = jnp.where((r0 == expert) | (r1 == expert), 1.0, 0.0)
    other = jnp.where(r0 == expert, r1, r0).astype(F32)
    mine = (lane // 4) % 2 == core

    def own_rows(v):
        moved = jnp.where(core == 0, pltpu.roll(v, 4, 1), pltpu.roll(v, 508, 1))
        return jnp.where(mine, v, moved)

    hit = own_rows(hit)
    other = own_rows(other)
    rank = jnp.zeros_like(hit)
    for d in range(1, 4):
        rank = rank + jnp.where(lane % 4 >= d, pltpu.roll(hit, d, 1), 0.0)
    srow, slane = iota((128, 256), 0), iota((128, 256), 1)
    fits = (srow // 64 == (slane // 4) % 2) & ((srow % 64) // 2 == slane // 8)
    sels, spreads = [], []
    for u in range(2):
        cols = slice(256 * u, 256 * (u + 1))
        sel = jnp.where(
            fits & (rank[:, cols] == (srow % 2).astype(F32)), jnp.broadcast_to(hit[:, cols], (128, 256)), 0.0
        )
        sels.append(sel.astype(BF16))
        spreads.append(jnp.transpose(sel).astype(BF16))
    other_t = jnp.transpose(jnp.broadcast_to(other, (128, 512)))
    wl = iota((512, 128), 1)
    pick = jnp.where(wl == 96 + expert, 1.0, 0.0) - jnp.where(wl == 96 + other_t.astype(jnp.int32), 1.0, 0.0)
    e_row, e_col = iota((128, 512), 0), iota((128, 512), 1)
    spread_e = jnp.where((e_row // 16 == e_col // 128) & (e_row % 16 == e_col % 16), 1.0, 0.0).astype(BF16)
    m_row, m_col = iota((512, 512), 0), iota((512, 512), 1)
    in_place = (m_row // 8) % 8 == (m_col // 16) % 8
    s_row, s_col = iota((32, 512), 0), iota((32, 512), 1)
    fold = jnp.where((s_col // 64 == s_row % 8) & (s_col % 8 == s_row // 8), 1.0, 0.0).astype(BF16)

    for i in range(4):
        c_wp[i].wait()
        got((pw_s, i))
    w64 = wp.reshape(64, 2048)
    w128 = jnp.concatenate([w64[:, :HALF], w64[:, HALF:]], axis=0)
    for part in range(3):
        walk_send(wm, part, 1, wm_s, wm_r)
    for part in range(3):
        got((tk_s, part, 4))
    proj = dot_nt(tb.reshape(512, HALF)[...], w128)
    proj = proj + pltpu.roll(pltpu.roll(proj, 508, 0), 64, 1)
    msg.reshape(512, 128)[...] = proj.astype(BF16)

    @pl.loop(1, 64)
    def _(j):
        to = (chip + j) % 64
        remote(msg.at[to], rcv.at[chip], a2_s, a2_r, 2 * to + core)

    expect(a2_s, rcv.at[0:63], a2_s, a2_r)
    rcv[chip] = msg[chip]
    for part in range(3):
        walk_send(wm, part, 2, wm_s, wm_r)

    wd[...] = jnp.zeros_like(wd)
    wdd[...] = jnp.zeros_like(wdd)
    for i in range(6):
        c_w[i].wait()
        got((pw_s, 4 + i))
    for c in range(2):
        for h in range(2):
            ls = slice(HALF * h, HALF * (h + 1))
            wd[256 * h + 48 * c : 256 * h + 48 * c + 44, :] = dg[c, :, ls]
            wd[256 * h + 128 + 48 * c : 256 * h + 128 + 48 * c + 44, :] = du[c, :, ls]
            wdd[128 * h + 48 * c : 128 * h + 48 * c + 44, :] = dd[c, :, ls]
    for h in range(2):
        ls = slice(HALF * h, HALF * (h + 1))
        brow = jnp.concatenate([br[8 * h + i : 8 * h + i + 1, :].astype(F32) for i in range(8)], axis=1)
        extra = jnp.concatenate([rt[:, ls].astype(F32), brow, jnp.zeros((7, HALF), F32)], axis=0)
        wd[256 * h + 96 : 256 * h + 112, :] = extra.astype(BF16)

    got(a2_s)
    wide = dot(rcv.reshape(512, 128)[...], spread_e)
    wide = jnp.where(in_place, wide, 0.0).astype(BF16)
    rows = dot(fold, wide)
    query, f_in, value, outgate = (rows[:, 128 * i : 128 * (i + 1)] for i in range(4))
    low = jnp.concatenate([lb[...]] * 4, axis=0)
    forget = low + (1.0 - low) * sigmoid(f_in)
    keyed = (1.0 - low) * sigmoid(-f_in)
    cols = jnp.transpose(jnp.concatenate([forget, keyed, query, query], axis=0))
    c_out = []
    for t in range(4):
        c_st[t].wait()
        for h in range(8):
            r = 8 * t + h
            fresh = cols[:, r : r + 1] * st[t, h] + cols[:, 32 + r : 33 + r] * value[r : r + 1, :]
            nst[t, h] = fresh
            rd[r : r + 1, :] = jnp.sum(fresh * cols[:, 64 + r : 65 + r], axis=0, keepdims=True)
        c_out.append(local(nst.at[t], nst_h.at[t], nsem.at[t]))
    read = rd[...]
    scaled = read * lax.rsqrt(jnp.mean(read * read, axis=1, keepdims=True) + HEAD_EPS) * hg[...]
    mx[core] = (scaled * (outgate * sigmoid(outgate))).astype(BF16).astype(F32)
    remote(mx.at[core], mx.at[core], mx_s.at[0], mx_r.at[0], partner)
    expect((mx_s, 0), mx.at[0], mx_s.at[0], mx_r.at[0])
    for part in range(3):
        got((wm_s, part, 2))
    got((mx_s, 0))
    mxv = mx.reshape(64, 128)
    lhs = jnp.concatenate([mxv[pl.ds(4 * core + i, 8, stride=8), :] for i in range(4)], axis=1).astype(BF16)
    mo = dot_nt(lhs, wm.reshape(2048, 512)[...])
    mos[0] = mo[:4]
    mos[1] = mo[4:]
    remote(mos.at[1 - core], mor, mx_s.at[1], mx_r.at[1], partner)
    expect((mx_s, 1), mor, mx_s.at[1], mx_r.at[1])
    mo = mos[core]
    got((mx_s, 1))
    mo = (mo + mor[...]).astype(BF16).astype(F32)
    pre = ALPHA * toks + mo
    center = jnp.mean(pre, axis=1, keepdims=True)
    var = jnp.mean(jnp.square(pre - center), axis=1, keepdims=True)
    normed = ((pre - center) * lax.rsqrt(var + NORM_EPS) * g1[...] + b1[...]).astype(BF16).astype(F32)
    nblk = jnp.concatenate([normed[:, :HALF], normed[:, HALF:]], axis=0)
    nb[own] = nblk.astype(BF16)

    for part in range(3):
        plane_send(nb, part, nb_s, nb_r)
    for g in (0, 1, 3, 2):
        for part in range(3):
            line_send(nb, part, g, nb_s, nb_r)
    for part in range(3):
        got((nb_s, part, 4))

    nbv = nb.reshape(512, HALF)
    for u in range(2):
        sel = dot(sels[u], nbv[256 * u : 256 * (u + 1), :]).astype(BF16)
        xe[64 * u : 64 * (u + 1), :HALF] = sel[:64]
        xe[64 * u : 64 * (u + 1), HALF:] = sel[64:]
    gate = dot_nt(xe[...], eg.reshape(896, 2048)[...])
    up = dot_nt(xe[...], eu.reshape(896, 2048)[...])
    hidden = (gate * sigmoid(gate) * up).astype(BF16)
    y2 = dot_nt(nbv[...], wd[...])
    first_half = (iota((512, 256), 0) // 4) % 2 == 0
    y = jnp.where(first_half, y2[:, :256], y2[:, 256:]).reshape(64, 8, 256)
    y = (y + pltpu.roll(y, 4, 1)).reshape(512, 256)
    yg = y[:, :128]
    weight = sigmoid(jnp.sum(yg * pick, axis=1, keepdims=True))
    branch = sigmoid(yg[:, 104:105])
    hd = yg * sigmoid(yg) * y[:, 128:] * branch
    top = (iota((512, 128), 0) // 4) % 2 == 0
    hdd = jnp.concatenate([jnp.where(top, hd, 0.0), jnp.where(top, 0.0, hd)], axis=1).astype(BF16)
    slots = dot(hidden, ed.reshape(896, 2048)[...]).astype(BF16)
    obv = ob.reshape(512, HALF)
    for u in range(2):
        ru = slice(256 * u, 256 * (u + 1))
        rows_u = jnp.concatenate([slots[64 * u : 64 * (u + 1), :HALF], slots[64 * u : 64 * (u + 1), HALF:]], axis=0)
        total = weight[ru] * dot(spreads[u], rows_u) + dot(hdd[ru], wdd[...])
        obv[ru, :] = total.astype(BF16)

    r1s, r2s, t1s = (r1a, r1b, r1c), (r2a, r2b, r2c), (t1a, t1b, t1c)
    spots = ((2, 0), (1, 1), (3, 2), (0, 3))
    for g, slot in spots:
        for part in range(3):
            d1, d2, _ = ORDERS[part]
            for k in (2, 1, 3):
                idx = region(part, {d1: (at[d1] + k) % 4, d2: (at[d2] + g) % 4})
                remote(
                    ob.at[idx + TAILS[part]], r1s[part].at[slot, k - 1], rs_s.at[part, slot], rs_r.at[part, slot],
                    peer({d1: k}),
                )
            expect((rs_s, part, slot), r1s[part].at[slot], rs_s.at[part, slot], rs_r.at[part, slot])
    for g, slot in spots:
        for part in range(3):
            d1, d2, d3 = ORDERS[part]
            got((rs_s, part, slot))
            idx = region(part, {d1: at[d1], d2: (at[d2] + g) % 4})
            total = ob[idx + TAILS[part]].astype(F32)
            for k in range(3):
                total = total + r1s[part][slot, k].astype(F32)
            t1s[part][slot] = total.astype(BF16)
            for k in (2, 1, 3, 0):
                if k or g:
                    remote(
                        t1s[part].at[slot, (at[d3] + k) % 4], r2s[part].at[4 * g + k - 1], rs_s.at[part, 4],
                        rs_r.at[part, 4], peer({d2: g, d3: k}),
                    )
    chans = []
    for part in range(3):
        d3 = ORDERS[part][2]
        take(r2s[part], rs_r.at[part, 4])
        total = t1s[part][3, at[d3]].astype(F32)
        for k in range(15):
            total = total + r2s[part][k].astype(F32)
        chans.append(total)
        sent[f"r{part}"] = functools.partial(take, r2s[part], rs_s.at[part, 4])
    z = ALPHA * nblk + jnp.concatenate(chans, axis=1)

    def both(v):
        v = jnp.broadcast_to(v, (8, 128))
        return (v + pltpu.roll(v, 4, 0))[:, 0:1]

    def by_half(ref):
        v = ref[...]
        return jnp.concatenate(
            [jnp.broadcast_to(v[:, :HALF], (4, HALF)), jnp.broadcast_to(v[:, HALF:], (4, HALF))], axis=0
        )

    center = both(jnp.sum(z, axis=1, keepdims=True)) * (1.0 / 2048)
    dev = z - center
    var = both(jnp.sum(dev * dev, axis=1, keepdims=True)) * (1.0 / 2048)
    res = dev * lax.rsqrt(var + NORM_EPS) * by_half(g2) + by_half(b2)
    outv[:, :HALF] = res[:4].astype(BF16)
    outv[:, HALF:] = res[4:].astype(BF16)
    c_out.append(local(outv, out_h, loc.at[0]))

    for c in c_out:
        c.wait()
    for wait in sent.values():
        wait()


def per_device(
    tokens, recurrent_state, query_weight, forget_weight, input_weight, outgate_weight, lower_bound, head_gain,
    mixout_weight, first_gain, first_bias, router_weight, branch_vector, dense_gate_weight, dense_up_weight,
    dense_down_weight, expert_gate_weight, expert_up_weight, expert_down_weight, second_gain, second_bias, routes,
):
    args = (
        tokens, recurrent_state, query_weight.T, forget_weight.T, input_weight.T, outgate_weight.T,
        lower_bound.reshape(8, 128), head_gain.reshape(1, 128), mixout_weight.T, first_gain.reshape(1, 2048),
        first_bias.reshape(1, 2048), router_weight.T, branch_vector.reshape(16, 128), dense_gate_weight.T,
        dense_up_weight.T, dense_down_weight, expert_gate_weight.T, expert_up_weight.T, expert_down_weight,
        second_gain.reshape(1, 2048), second_bias.reshape(1, 2048), routes.T,
    )
    lanes = [p.stop - p.start for p in LANES]
    V = pltpu.VMEM
    sem = pltpu.SemaphoreType.DMA
    scratch = [
        V((4, 2048), BF16), V((4, 2048), BF16), V((4, 8, 128, 128), F32), V((4, 8, 128, 128), F32), V((4, 2, 8, 2048), BF16),
        V((8, 128), F32), V((1, 128), F32), V((4, 4, 4, 2, 16, 512), BF16), V((1, 2048), F32), V((1, 2048), F32),
        V((8, 2048), BF16), V((16, 128), BF16), V((2, 44, 2048), BF16), V((2, 44, 2048), BF16),
        V((2, 44, 2048), BF16), V((2, 448, 2048), BF16), V((2, 448, 2048), BF16), V((2, 448, 2048), BF16),
        V((1, 2048), F32), V((1, 2048), F32), V((2, 512), jnp.int32),
        V((4, 4, 4, 8, HALF), BF16), V((4, 4, 4, 8, HALF), BF16), V((64, 8, 128), BF16), V((64, 8, 128), BF16),
        V((4, 4, 4, 8, HALF), BF16), V((128, 2048), BF16), V((512, HALF), BF16), V((256, HALF), BF16),
        V((32, 128), F32),
        *[V((4, 3, 4, 8, n), BF16) for n in lanes], *[V((15, 8, n), BF16) for n in lanes],
        *[V((4, 4, 8, n), BF16) for n in lanes],
        V((2, 32, 128), F32), V((2, 4, 2048), F32), V((4, 2048), F32),
        sem((21,)), sem((4,)), sem((4,)), sem((10,)), sem((10,)), sem((3, 3)), sem((3, 3)), sem(()), sem(()),
        sem((2,)), sem((2,)), sem((3, 5)), sem((3, 5)), sem((3, 5)), sem((3, 5)), sem(()), sem(()), sem((3, 5)), sem((3, 5)),
    ]
    hbm = pl.BlockSpec(memory_space=pltpu.HBM)
    free = pl.BlockSpec(memory_space=pl.ANY)
    return pl.pallas_call(
        kernel,
        out_shape=(jax.ShapeDtypeStruct((4, 2048), BF16), jax.ShapeDtypeStruct((4, 8, 128, 128), F32)),
        in_specs=[hbm] * 22,
        out_specs=(free, free),
        scratch_shapes=scratch,
        compiler_params=pltpu.CompilerParams(
            collective_id=0, has_side_effects=True, vmem_limit_bytes=60 * 1024 * 1024
        ),
        name="layer",
    )(*args)


def solution(mesh):
    ep = "ep"
    cols, rows = P(None, ep), P(ep, None)
    return jax.shard_map(
        per_device,
        mesh=mesh,
        in_specs=(
            rows, P(ep, None, None, None), cols, cols, cols, cols, P(), P(), cols, P(), P(), P(), P(),
            cols, cols, rows, cols, cols, rows, P(), P(), P(),
        ),
        out_specs=(rows, P(ep, None, None, None)),
        check_vma=False,
    )
```

```python
import functools

import jax
import jax.numpy as jnp
from jax import lax
from jax.experimental import pallas as pl
from jax.experimental.pallas import tpu as pltpu
from jax.sharding import PartitionSpec as P

ALPHA = 8.0**0.25
NORM_EPS = 1e-05
HEAD_EPS = 1e-06
HALF = 1024
F32 = jnp.float32
BF16 = jnp.bfloat16
ALL = slice(None)
ORDERS = ((2, 1, 0), (1, 0, 2), (0, 2, 1))
LANES = (slice(0, 384), slice(384, 768), slice(768, 1024))
TAILS = tuple((ALL, lanes) for lanes in LANES)
WTAILS = ((ALL, slice(0, 8), slice(0, 384)), (ALL, slice(8, 16), slice(0, 384)), (ALL, ALL, slice(384, 512)))
NT = (((1,), (1,)), ((), ()))


def dot(a, b):
    return jnp.dot(a, b, preferred_element_type=F32)


def dot_nt(a, b):
    return lax.dot_general(a, b, NT, preferred_element_type=F32)


def iota(shape, dim):
    return lax.broadcasted_iota(jnp.int32, shape, dim)


def id_of(part):
    return part if isinstance(part, int) else id(part)


def sigmoid(a):
    return 1.0 / (1.0 + jnp.exp(-a))


def kernel(
    tok_h, state_h, wq_h, wf_h, wi_h, wo_h, lb_h, hg_h, wm_h, g1_h, b1_h, router_h, branch_h,
    dg_h, du_h, dd_h, eg_h, eu_h, ed_h, g2_h, b2_h, routes_h,
    out_h, nst_h,
    tokv, outv, st, nst, wp, lb, hg, wm, g1, b1, rt, br, dg, du, dd, eg, eu, ed, g2, b2, rts,
    tb, nb, msg, rcv, ob, xe, wd, wdd, rd,
    r1a, r1b, r1c, r2a, r2b, r2c, t1a, t1b, t1c, mx, mos, mor,
    loc, stsem, nsem, pw_s, pw_r, wm_s, wm_r, wmx_s, wmx_r, mx_s, mx_r, tk_s, tk_r, nb_s, nb_r, a2_s, a2_r, rs_s, rs_r,
):
    me = lax.axis_index("ep")
    core = me % 2
    chip = me // 2
    at = (chip // 16, (chip // 4) % 4, chip % 4)
    partner = me + 1 - 2 * core

    def peer(steps):
        c = [(at[d] + steps[d]) % 4 if steps.get(d) else at[d] for d in range(3)]
        return 2 * ((c[0] * 4 + c[1]) * 4 + c[2]) + core

    def remote(src, dst, ss, rs, dev):
        pltpu.make_async_remote_copy(
            src_ref=src, dst_ref=dst, send_sem=ss, recv_sem=rs, device_id=(dev,),
            device_id_type=pl.DeviceIdType.MESH,
        ).start()

    sent, due = {}, {}

    def local(src, dst, sem):
        cp = pltpu.make_async_copy(src, dst, sem)
        cp.start()
        return cp

    def expect(key, ref, ss, rs):
        key = tuple(map(id_of, key)) if isinstance(key, tuple) else id_of(key)
        sent[key] = functools.partial(take, ref, ss)
        due[key] = functools.partial(take, ref, rs)

    def got(key):
        key = tuple(map(id_of, key)) if isinstance(key, tuple) else id_of(key)
        due.pop(key)()

    def take(ref, sem):
        pltpu.make_async_copy(ref, ref, sem).wait()

    own = (at[0], at[1], at[2])
    c_tok = local(tok_h, tokv, loc.at[0])
    c_wp = [local(w, wp.at[i, core], loc.at[1 + i]) for i, w in enumerate((wq_h, wf_h, wi_h, wo_h))]
    half_own = pl.ds(pl.multiple_of(core * 512, 512), 512)
    c_wm = local(wm_h.at[:, half_own], wm.at[own + (core,)], loc.at[5])
    c_small = [
        local(a, b, loc.at[6 + i])
        for i, (a, b) in enumerate(
            ((lb_h, lb), (hg_h, hg), (g1_h, g1), (b1_h, b1), (router_h, rt), (branch_h, br),
             (g2_h, g2), (b2_h, b2), (routes_h, rts))
        )
    ]
    barrier = pltpu.get_barrier_semaphore()
    steps = [{d1: k1, d2: k2} for d1, d2 in ((0, 1), (0, 2), (1, 2)) for k1 in (2, 1, 3) for k2 in (2, 1, 3)]
    steps += [{d: k} for d in range(3) for k in (2, 1, 3)]
    for step in steps:
        pl.semaphore_signal(barrier, inc=1, device_id=(peer(step),), device_id_type=pl.DeviceIdType.MESH)
    pl.semaphore_signal(barrier, inc=1, device_id=(partner,), device_id_type=pl.DeviceIdType.MESH)
    c_tok.wait()
    toks = tokv[...].astype(F32)
    tblk = jnp.concatenate([toks[:, :HALF], toks[:, HALF:]], axis=0).astype(BF16)
    tb[own] = tblk
    pl.semaphore_wait(barrier, 37)

    def region(part, fixed):
        return tuple(fixed.get(d, ALL) for d in range(3))

    def blocks(buf, tail, count):
        idx = {3: (0, 0, slice(0, 3)), 4: (0, 0, ALL), 12: (0, slice(0, 3), ALL), 48: (slice(0, 3), ALL, ALL)}[count]
        return buf.at[idx + tail]

    def plane_send(buf, part, ss, rs):
        d1, d2, _ = ORDERS[part]
        ref = buf.at[own + TAILS[part]]
        for k2 in (2, 1, 3, 0):
            for k1 in (2, 1, 3, 0):
                if k1 or k2:
                    remote(ref, ref, ss.at[part, k2], rs.at[part, (4 - k2) % 4], peer({d1: k1, d2: k2}))
        for g in range(4):
            expect((ss, part, g), blocks(buf, TAILS[part], 4 if g else 3), ss.at[part, g], rs.at[part, g])

    def line_send(buf, part, g, ss, rs):
        d1, d2, d3 = ORDERS[part]
        got((ss, part, g))
        idx = region(part, {d2: (at[d2] + g) % 4, d3: at[d3]})
        ref = buf.at[idx + TAILS[part]]
        for k in (2, 1, 3):
            remote(ref, ref, ss.at[part, 4], rs.at[part, 4], peer({d3: k}))
        if g == 2:
            expect((ss, part, 4), blocks(buf, TAILS[part], 48), ss.at[part, 4], rs.at[part, 4])

    def walk_send(part, phase):
        d1, d2, d3 = ORDERS[part]
        if phase:
            got((wm_s, part, 0))
        ref = wm.at[region(part, {d: at[d] for d in (d1, d2, d3)[phase:]}) + WTAILS[part]]
        for k in (2, 1, 3):
            sems = (0, 0) if phase == 0 else (k, 4 - k)
            remote(ref, ref, wm_s.at[part, sems[0]], wm_r.at[part, sems[1]], peer({(d1, d2)[phase]: k}))
        for g in range(1, 4) if phase else (0,):
            expect(
                (wm_s, part, g), blocks(wm, WTAILS[part], 4 if phase else 3), wm_s.at[part, g], wm_r.at[part, g]
            )

    def walk_last(part, g):
        _, d2, d3 = ORDERS[part]
        if g:
            got((wm_s, part, g))
        ref = wm.at[region(part, {d2: (at[d2] + g) % 4, d3: at[d3]}) + WTAILS[part]]
        for k in (2, 1, 3):
            remote(ref, ref, wm_s.at[part, 4], wm_r.at[part, 4], peer({d3: k}))
        if g == 2:
            expect((wm_s, part, 4), blocks(wm, WTAILS[part], 48), wm_s.at[part, 4], wm_r.at[part, 4])

    for part in range(3):
        plane_send(tb, part, tk_s, tk_r)
    half_in = pl.ds(pl.multiple_of((1 - core) * 512, 512), 512)
    remote(wm_h.at[:, half_in], wm.at[own + (core,)], wmx_s, wmx_r, partner)
    expect(wmx_s, wm.at[own + (0,)], wmx_s, wmx_r)
    for i, w in enumerate((wq_h, wf_h, wi_h, wo_h)):
        remote(w, wp.at[i, core], pw_s.at[i], pw_r.at[i], partner)
        expect((pw_s, i), wp.at[i, 0], pw_s.at[i], pw_r.at[i])
    c_st = [local(state_h.at[t], st.at[t], stsem.at[t]) for t in range(4)]
    c_w = []
    big = ((dg_h, dg), (du_h, du), (dd_h, dd), (eg_h, eg), (eu_h, eu), (ed_h, ed))
    for i, (a, b) in enumerate(big):
        c_w.append(local(a, b.at[core], loc.at[15 + i]))
    for part in range(3):
        line_send(tb, part, 0, tk_s, tk_r)
    c_wm.wait()
    got(wmx_s)
    for part in range(3):
        walk_send(part, 0)
    for g in (1, 3, 2):
        for part in range(3):
            line_send(tb, part, g, tk_s, tk_r)
    for part in range(3):
        walk_send(part, 1)
        walk_last(part, 0)
    for i, (a, b) in enumerate(big):
        remote(a, b.at[core], pw_s.at[4 + i], pw_r.at[4 + i], partner)
        expect((pw_s, 4 + i), b.at[0], pw_s.at[4 + i], pw_r.at[4 + i])

    for c in c_small:
        c.wait()
    expert = chip // 8
    r0 = rts[0:1, :]
    r1 = rts[1:2, :]
    lane = iota((1, 512), 1)
    hit = jnp.where((r0 == expert) | (r1 == expert), 1.0, 0.0)
    other = jnp.where(r0 == expert, r1, r0).astype(F32)
    mine = (lane // 4) % 2 == core

    def own_rows(v):
        moved = jnp.where(core == 0, pltpu.roll(v, 4, 1), pltpu.roll(v, 508, 1))
        return jnp.where(mine, v, moved)

    hit = own_rows(hit)
    other = own_rows(other)
    rank = jnp.zeros_like(hit)
    for d in range(1, 4):
        rank = rank + jnp.where(lane % 4 >= d, pltpu.roll(hit, d, 1), 0.0)
    srow, slane = iota((128, 256), 0), iota((128, 256), 1)
    fits = (srow // 64 == (slane // 4) % 2) & ((srow % 64) // 2 == slane // 8)
    sels, spreads = [], []
    for u in range(2):
        cols = slice(256 * u, 256 * (u + 1))
        sel = jnp.where(
            fits & (rank[:, cols] == (srow % 2).astype(F32)), jnp.broadcast_to(hit[:, cols], (128, 256)), 0.0
        )
        sels.append(sel.astype(BF16))
        spreads.append(jnp.transpose(sel).astype(BF16))
    other_t = jnp.transpose(jnp.broadcast_to(other, (128, 512)))
    wl = iota((512, 128), 1)
    pick = jnp.where(wl == 96 + expert, 1.0, 0.0) - jnp.where(wl == 96 + other_t.astype(jnp.int32), 1.0, 0.0)
    e_row, e_col = iota((128, 512), 0), iota((128, 512), 1)
    spread_e = jnp.where((e_row // 16 == e_col // 128) & (e_row % 16 == e_col % 16), 1.0, 0.0).astype(BF16)
    m_row, m_col = iota((512, 512), 0), iota((512, 512), 1)
    in_place = (m_row // 8) % 8 == (m_col // 16) % 8
    s_row, s_col = iota((32, 512), 0), iota((32, 512), 1)
    fold = jnp.where((s_col // 64 == s_row % 8) & (s_col % 8 == s_row // 8), 1.0, 0.0).astype(BF16)

    for i in range(4):
        c_wp[i].wait()
        got((pw_s, i))
    w64 = wp.reshape(64, 2048)
    w128 = jnp.concatenate([w64[:, :HALF], w64[:, HALF:]], axis=0)
    for part in range(3):
        got((tk_s, part, 4))
    proj = dot_nt(tb.reshape(512, HALF)[...], w128)
    proj = proj + pltpu.roll(pltpu.roll(proj, 508, 0), 64, 1)
    msg.reshape(512, 128)[...] = proj.astype(BF16)

    @pl.loop(1, 64)
    def _(j):
        to = (chip + j) % 64
        remote(msg.at[to], rcv.at[chip], a2_s, a2_r, 2 * to + core)

    expect(a2_s, rcv.at[0:63], a2_s, a2_r)
    rcv[chip] = msg[chip]
    for g in (1, 3, 2):
        for part in range(3):
            walk_last(part, g)

    wd[...] = jnp.zeros_like(wd)
    wdd[...] = jnp.zeros_like(wdd)
    for i in range(6):
        c_w[i].wait()
        got((pw_s, 4 + i))
    for c in range(2):
        for h in range(2):
            ls = slice(HALF * h, HALF * (h + 1))
            wd[256 * h + 48 * c : 256 * h + 48 * c + 44, :] = dg[c, :, ls]
            wd[256 * h + 128 + 48 * c : 256 * h + 128 + 48 * c + 44, :] = du[c, :, ls]
            wdd[128 * h + 48 * c : 128 * h + 48 * c + 44, :] = dd[c, :, ls]
    for h in range(2):
        ls = slice(HALF * h, HALF * (h + 1))
        brow = jnp.concatenate([br[8 * h + i : 8 * h + i + 1, :].astype(F32) for i in range(8)], axis=1)
        extra = jnp.concatenate([rt[:, ls].astype(F32), brow, jnp.zeros((7, HALF), F32)], axis=0)
        wd[256 * h + 96 : 256 * h + 112, :] = extra.astype(BF16)

    got(a2_s)
    wide = dot(rcv.reshape(512, 128)[...], spread_e)
    wide = jnp.where(in_place, wide, 0.0).astype(BF16)
    rows = dot(fold, wide)
    query, f_in, value, outgate = (rows[:, 128 * i : 128 * (i + 1)] for i in range(4))
    low = jnp.concatenate([lb[...]] * 4, axis=0)
    forget = low + (1.0 - low) * sigmoid(f_in)
    keyed = (1.0 - low) * sigmoid(-f_in)
    cols = jnp.transpose(jnp.concatenate([forget, keyed, query, query], axis=0))
    c_out = []
    for t in range(4):
        c_st[t].wait()
        for h in range(8):
            r = 8 * t + h
            fresh = cols[:, r : r + 1] * st[t, h] + cols[:, 32 + r : 33 + r] * value[r : r + 1, :]
            nst[t, h] = fresh
            rd[r : r + 1, :] = jnp.sum(fresh * cols[:, 64 + r : 65 + r], axis=0, keepdims=True)
        c_out.append(local(nst.at[t], nst_h.at[t], nsem.at[t]))
    read = rd[...]
    scaled = read * lax.rsqrt(jnp.mean(read * read, axis=1, keepdims=True) + HEAD_EPS) * hg[...]
    mx[core] = (scaled * (outgate * sigmoid(outgate))).astype(BF16).astype(F32)
    remote(mx.at[core], mx.at[core], mx_s.at[0], mx_r.at[0], partner)
    expect((mx_s, 0), mx.at[0], mx_s.at[0], mx_r.at[0])
    for part in range(3):
        got((wm_s, part, 4))
    got((mx_s, 0))
    mxv = mx.reshape(64, 128)
    lhs = jnp.concatenate([mxv[pl.ds(4 * core + i, 8, stride=8), :] for i in range(4)], axis=1).astype(BF16)
    mo = dot_nt(lhs, wm.reshape(2048, 512)[...])
    mos[0] = mo[:4]
    mos[1] = mo[4:]
    remote(mos.at[1 - core], mor, mx_s.at[1], mx_r.at[1], partner)
    expect((mx_s, 1), mor, mx_s.at[1], mx_r.at[1])
    mo = mos[core]
    got((mx_s, 1))
    mo = (mo + mor[...]).astype(BF16).astype(F32)
    pre = ALPHA * toks + mo
    center = jnp.mean(pre, axis=1, keepdims=True)
    var = jnp.mean(jnp.square(pre - center), axis=1, keepdims=True)
    normed = ((pre - center) * lax.rsqrt(var + NORM_EPS) * g1[...] + b1[...]).astype(BF16).astype(F32)
    nblk = jnp.concatenate([normed[:, :HALF], normed[:, HALF:]], axis=0)
    nb[own] = nblk.astype(BF16)

    for part in range(3):
        plane_send(nb, part, nb_s, nb_r)
    for g in (0, 1, 3, 2):
        for part in range(3):
            line_send(nb, part, g, nb_s, nb_r)
    for part in range(3):
        got((nb_s, part, 4))

    nbv = nb.reshape(512, HALF)
    for u in range(2):
        sel = dot(sels[u], nbv[256 * u : 256 * (u + 1), :]).astype(BF16)
        xe[64 * u : 64 * (u + 1), :HALF] = sel[:64]
        xe[64 * u : 64 * (u + 1), HALF:] = sel[64:]
    gate = dot_nt(xe[...], eg.reshape(896, 2048)[...])
    up = dot_nt(xe[...], eu.reshape(896, 2048)[...])
    hidden = (gate * sigmoid(gate) * up).astype(BF16)
    y2 = dot_nt(nbv[...], wd[...])
    first_half = (iota((512, 256), 0) // 4) % 2 == 0
    y = jnp.where(first_half, y2[:, :256], y2[:, 256:]).reshape(64, 8, 256)
    y = (y + pltpu.roll(y, 4, 1)).reshape(512, 256)
    yg = y[:, :128]
    weight = sigmoid(jnp.sum(yg * pick, axis=1, keepdims=True))
    branch = sigmoid(yg[:, 104:105])
    hd = yg * sigmoid(yg) * y[:, 128:] * branch
    top = (iota((512, 128), 0) // 4) % 2 == 0
    hdd = jnp.concatenate([jnp.where(top, hd, 0.0), jnp.where(top, 0.0, hd)], axis=1).astype(BF16)
    slots = dot(hidden, ed.reshape(896, 2048)[...]).astype(BF16)
    obv = ob.reshape(512, HALF)
    for u in range(2):
        ru = slice(256 * u, 256 * (u + 1))
        rows_u = jnp.concatenate([slots[64 * u : 64 * (u + 1), :HALF], slots[64 * u : 64 * (u + 1), HALF:]], axis=0)
        total = weight[ru] * dot(spreads[u], rows_u) + dot(hdd[ru], wdd[...])
        obv[ru, :] = total.astype(BF16)

    r1s, r2s, t1s = (r1a, r1b, r1c), (r2a, r2b, r2c), (t1a, t1b, t1c)
    spots = ((2, 0), (1, 1), (3, 2), (0, 3))
    for g, slot in spots:
        for part in range(3):
            d1, d2, _ = ORDERS[part]
            for k in (2, 1, 3):
                idx = region(part, {d1: (at[d1] + k) % 4, d2: (at[d2] + g) % 4})
                remote(
                    ob.at[idx + TAILS[part]], r1s[part].at[slot, k - 1], rs_s.at[part, slot], rs_r.at[part, slot],
                    peer({d1: k}),
                )
            expect((rs_s, part, slot), r1s[part].at[slot], rs_s.at[part, slot], rs_r.at[part, slot])
    for g, slot in spots:
        for part in range(3):
            d1, d2, d3 = ORDERS[part]
            got((rs_s, part, slot))
            idx = region(part, {d1: at[d1], d2: (at[d2] + g) % 4})
            total = ob[idx + TAILS[part]].astype(F32)
            for k in range(3):
                total = total + r1s[part][slot, k].astype(F32)
            t1s[part][slot] = total.astype(BF16)
            for k in (2, 1, 3, 0):
                if k or g:
                    remote(
                        t1s[part].at[slot, (at[d3] + k) % 4], r2s[part].at[4 * g + k - 1], rs_s.at[part, 4],
                        rs_r.at[part, 4], peer({d2: g, d3: k}),
                    )
    chans = []
    for part in range(3):
        d3 = ORDERS[part][2]
        take(r2s[part], rs_r.at[part, 4])
        total = t1s[part][3, at[d3]].astype(F32)
        for k in range(15):
            total = total + r2s[part][k].astype(F32)
        chans.append(total)
        sent[f"r{part}"] = functools.partial(take, r2s[part], rs_s.at[part, 4])
    z = ALPHA * nblk + jnp.concatenate(chans, axis=1)

    def both(v):
        v = jnp.broadcast_to(v, (8, 128))
        return (v + pltpu.roll(v, 4, 0))[:, 0:1]

    def by_half(ref):
        v = ref[...]
        return jnp.concatenate(
            [jnp.broadcast_to(v[:, :HALF], (4, HALF)), jnp.broadcast_to(v[:, HALF:], (4, HALF))], axis=0
        )

    center = both(jnp.sum(z, axis=1, keepdims=True)) * (1.0 / 2048)
    dev = z - center
    var = both(jnp.sum(dev * dev, axis=1, keepdims=True)) * (1.0 / 2048)
    res = dev * lax.rsqrt(var + NORM_EPS) * by_half(g2) + by_half(b2)
    outv[:, :HALF] = res[:4].astype(BF16)
    outv[:, HALF:] = res[4:].astype(BF16)
    c_out.append(local(outv, out_h, loc.at[0]))

    for c in c_out:
        c.wait()
    for wait in sent.values():
        wait()


def closing(a_h, s_h, out_h, nst_h, av, sv, into, out):
    ins = [pltpu.make_async_copy(s_h.at[t], sv.at[t], into.at[t]) for t in range(4)]
    ins.append(pltpu.make_async_copy(a_h, av, into.at[4]))
    outs = [pltpu.make_async_copy(sv.at[t], nst_h.at[t], out.at[t]) for t in range(4)]
    outs.append(pltpu.make_async_copy(av, out_h, out.at[4]))
    for cp in ins:
        cp.start()
    for cp, back in zip(ins, outs):
        cp.wait()
        back.start()
    for back in outs:
        back.wait()


def per_device(
    tokens, recurrent_state, query_weight, forget_weight, input_weight, outgate_weight, lower_bound, head_gain,
    mixout_weight, first_gain, first_bias, router_weight, branch_vector, dense_gate_weight, dense_up_weight,
    dense_down_weight, expert_gate_weight, expert_up_weight, expert_down_weight, second_gain, second_bias, routes,
):
    args = (
        tokens, recurrent_state, query_weight.T, forget_weight.T, input_weight.T, outgate_weight.T,
        lower_bound.reshape(8, 128), head_gain.reshape(1, 128), mixout_weight.T, first_gain.reshape(1, 2048),
        first_bias.reshape(1, 2048), router_weight.T, branch_vector.reshape(16, 128), dense_gate_weight.T,
        dense_up_weight.T, dense_down_weight, expert_gate_weight.T, expert_up_weight.T, expert_down_weight,
        second_gain.reshape(1, 2048), second_bias.reshape(1, 2048), routes.T,
    )
    lanes = [p.stop - p.start for p in LANES]
    V = pltpu.VMEM
    sem = pltpu.SemaphoreType.DMA
    scratch = [
        V((4, 2048), BF16), V((4, 2048), BF16), V((4, 8, 128, 128), F32), V((4, 8, 128, 128), F32), V((4, 2, 8, 2048), BF16),
        V((8, 128), F32), V((1, 128), F32), V((4, 4, 4, 2, 16, 512), BF16), V((1, 2048), F32), V((1, 2048), F32),
        V((8, 2048), BF16), V((16, 128), BF16), V((2, 44, 2048), BF16), V((2, 44, 2048), BF16),
        V((2, 44, 2048), BF16), V((2, 448, 2048), BF16), V((2, 448, 2048), BF16), V((2, 448, 2048), BF16),
        V((1, 2048), F32), V((1, 2048), F32), V((2, 512), jnp.int32),
        V((4, 4, 4, 8, HALF), BF16), V((4, 4, 4, 8, HALF), BF16), V((64, 8, 128), BF16), V((64, 8, 128), BF16),
        V((4, 4, 4, 8, HALF), BF16), V((128, 2048), BF16), V((512, HALF), BF16), V((256, HALF), BF16),
        V((32, 128), F32),
        *[V((4, 3, 4, 8, n), BF16) for n in lanes], *[V((15, 8, n), BF16) for n in lanes],
        *[V((4, 4, 8, n), BF16) for n in lanes],
        V((2, 32, 128), F32), V((2, 4, 2048), F32), V((4, 2048), F32),
        sem((21,)), sem((4,)), sem((4,)), sem((10,)), sem((10,)), sem((3, 5)), sem((3, 5)), sem(()), sem(()),
        sem((2,)), sem((2,)), sem((3, 5)), sem((3, 5)), sem((3, 5)), sem((3, 5)), sem(()), sem(()), sem((3, 5)), sem((3, 5)),
    ]
    hbm = pl.BlockSpec(memory_space=pltpu.HBM)
    free = pl.BlockSpec(memory_space=pl.ANY)
    shapes = (jax.ShapeDtypeStruct((4, 2048), BF16), jax.ShapeDtypeStruct((4, 8, 128, 128), F32))
    res = pl.pallas_call(
        kernel,
        out_shape=shapes,
        in_specs=[hbm] * 22,
        out_specs=(free, free),
        scratch_shapes=scratch,
        compiler_params=pltpu.CompilerParams(
            collective_id=0, has_side_effects=True, vmem_limit_bytes=60 * 1024 * 1024
        ),
        name="layer",
    )(*args)
    return pl.pallas_call(
        closing,
        out_shape=shapes,
        in_specs=[free] * 2,
        out_specs=(free, free),
        scratch_shapes=[V((4, 2048), BF16), V((4, 8, 128, 128), F32), sem((5,)), sem((5,))],
        compiler_params=pltpu.CompilerParams(vmem_limit_bytes=60 * 1024 * 1024),
        name="closing",
    )(*res)


def solution(mesh):
    ep = "ep"
    cols, rows = P(None, ep), P(ep, None)
    return jax.shard_map(
        per_device,
        mesh=mesh,
        in_specs=(
            rows, P(ep, None, None, None), cols, cols, cols, cols, P(), P(), cols, P(), P(), P(), P(),
            cols, cols, rows, cols, cols, rows, P(), P(), P(),
        ),
        out_specs=(rows, P(ep, None, None, None)),
        check_vma=False,
    )
```

```python
import functools

import jax
import jax.numpy as jnp
from jax import lax
from jax.experimental import pallas as pl
from jax.experimental.pallas import tpu as pltpu
from jax.sharding import PartitionSpec as P

ALPHA = 8.0**0.25
NORM_EPS = 1e-05
HEAD_EPS = 1e-06
HALF = 1024
F32 = jnp.float32
BF16 = jnp.bfloat16
ALL = slice(None)
ORDERS = ((2, 1, 0), (1, 0, 2), (0, 2, 1))
LANES = (slice(0, 384), slice(384, 768), slice(768, 1024))
TAILS = tuple((ALL, lanes) for lanes in LANES)
WTAILS = ((ALL, slice(0, 8), slice(0, 384)), (ALL, slice(8, 16), slice(0, 384)), (ALL, ALL, slice(384, 512)))
NT = (((1,), (1,)), ((), ()))


def dot(a, b):
    return jnp.dot(a, b, preferred_element_type=F32)


def dot_nt(a, b):
    return lax.dot_general(a, b, NT, preferred_element_type=F32)


def iota(shape, dim):
    return lax.broadcasted_iota(jnp.int32, shape, dim)


def id_of(part):
    return part if isinstance(part, int) else id(part)


def sigmoid(a):
    return 1.0 / (1.0 + jnp.exp(-a))


def kernel(
    tok_h, state_h, wq_h, wf_h, wi_h, wo_h, lb_h, hg_h, wm_h, g1_h, b1_h, router_h, branch_h,
    dg_h, du_h, dd_h, eg_h, eu_h, ed_h, g2_h, b2_h, routes_h,
    out_h, nst_h,
    tokv, outv, st, nst, wp, lb, hg, wm, g1, b1, rt, br, dg, du, dd, eg, eu, ed, g2, b2, rts,
    tb, nb, msg, rcv, ob, xe, wd, wdd, rd,
    r1a, r1b, r1c, r2a, r2b, r2c, t1a, t1b, t1c, mx, mos, mor,
    loc, stsem, nsem, pw_s, pw_r, wm_s, wm_r, wmx_s, wmx_r, mx_s, mx_r, tk_s, tk_r, nb_s, nb_r, a2_s, a2_r, rs_s, rs_r,
):
    me = lax.axis_index("ep")
    core = me % 2
    chip = me // 2
    at = (chip // 16, (chip // 4) % 4, chip % 4)
    partner = me + 1 - 2 * core

    def peer(steps):
        c = [(at[d] + steps[d]) % 4 if steps.get(d) else at[d] for d in range(3)]
        return 2 * ((c[0] * 4 + c[1]) * 4 + c[2]) + core

    def remote(src, dst, ss, rs, dev):
        pltpu.make_async_remote_copy(
            src_ref=src, dst_ref=dst, send_sem=ss, recv_sem=rs, device_id=(dev,),
            device_id_type=pl.DeviceIdType.MESH,
        ).start()

    sent, due = {}, {}

    def local(src, dst, sem):
        cp = pltpu.make_async_copy(src, dst, sem)
        cp.start()
        return cp

    def expect(key, ref, ss, rs):
        key = tuple(map(id_of, key)) if isinstance(key, tuple) else id_of(key)
        sent[key] = functools.partial(take, ref, ss)
        due[key] = functools.partial(take, ref, rs)

    def got(key):
        key = tuple(map(id_of, key)) if isinstance(key, tuple) else id_of(key)
        due.pop(key)()

    def take(ref, sem):
        pltpu.make_async_copy(ref, ref, sem).wait()

    own = (at[0], at[1], at[2])
    barrier = pltpu.get_barrier_semaphore()
    for step in [{d: k} for d in range(3) for k in (2, 1, 3)]:
        pl.semaphore_signal(barrier, inc=1, device_id=(peer(step),), device_id_type=pl.DeviceIdType.MESH)
    pl.semaphore_signal(barrier, inc=1, device_id=(partner,), device_id_type=pl.DeviceIdType.MESH)
    c_tok = local(tok_h, tokv, loc.at[0])
    half_own = pl.ds(pl.multiple_of(core * 512, 512), 512)
    c_wm = local(wm_h.at[:, half_own], wm.at[own + (core,)], loc.at[5])
    c_wp = [local(w, wp.at[i, core], loc.at[1 + i]) for i, w in enumerate((wq_h, wf_h, wi_h, wo_h))]
    c_tok.wait()
    toks = tokv[...].astype(F32)
    tblk = jnp.concatenate([toks[:, :HALF], toks[:, HALF:]], axis=0).astype(BF16)
    tb[own] = tblk
    pl.semaphore_wait(barrier, 10)

    def region(part, fixed):
        return tuple(fixed.get(d, ALL) for d in range(3))

    def blocks(buf, tail, count):
        idx = {3: (0, 0, slice(0, 3)), 4: (0, 0, ALL), 12: (0, slice(0, 3), ALL), 48: (slice(0, 3), ALL, ALL)}[count]
        return buf.at[idx + tail]

    def plane_send(buf, part, ss, rs):
        d1, d2, _ = ORDERS[part]
        ref = buf.at[own + TAILS[part]]
        for k2 in (0, 1, 3, 2):
            for k1 in (1, 3, 2, 0):
                if k1 or k2:
                    remote(ref, ref, ss.at[part, k2], rs.at[part, (4 - k2) % 4], peer({d1: k1, d2: k2}))
        for g in range(4):
            expect((ss, part, g), blocks(buf, TAILS[part], 4 if g else 3), ss.at[part, g], rs.at[part, g])

    def line_send(buf, part, g, ss, rs):
        d1, d2, d3 = ORDERS[part]
        got((ss, part, g))
        idx = region(part, {d2: (at[d2] + g) % 4, d3: at[d3]})
        ref = buf.at[idx + TAILS[part]]
        for k in (2, 1, 3):
            remote(ref, ref, ss.at[part, 4], rs.at[part, 4], peer({d3: k}))
        if g == 2:
            expect((ss, part, 4), blocks(buf, TAILS[part], 48), ss.at[part, 4], rs.at[part, 4])

    def walk_send(buf, tails, part, phase, ss, rs):
        d1, d2, d3 = ORDERS[part]
        if phase:
            got((ss, part, 0))
        ref = buf.at[region(part, {d: at[d] for d in (d1, d2, d3)[phase:]}) + tails[part]]
        for k in (2, 1, 3):
            sems = (0, 0) if phase == 0 else (k, 4 - k)
            remote(ref, ref, ss.at[part, sems[0]], rs.at[part, sems[1]], peer({(d1, d2)[phase]: k}))
        for g in range(1, 4) if phase else (0,):
            expect((ss, part, g), blocks(buf, tails[part], 4 if phase else 3), ss.at[part, g], rs.at[part, g])

    def walk_last(buf, tails, part, g, ss, rs):
        _, d2, d3 = ORDERS[part]
        if g:
            got((ss, part, g))
        ref = buf.at[region(part, {d2: (at[d2] + g) % 4, d3: at[d3]}) + tails[part]]
        for k in (2, 1, 3):
            remote(ref, ref, ss.at[part, 4], rs.at[part, 4], peer({d3: k}))
        if g == 2:
            expect((ss, part, 4), blocks(buf, tails[part], 48), ss.at[part, 4], rs.at[part, 4])

    of_wm, of_tb = (wm, WTAILS), (tb, TAILS)
    for part in range(3):
        walk_send(*of_tb, part, 0, tk_s, tk_r)
    half_in = pl.ds(pl.multiple_of((1 - core) * 512, 512), 512)
    remote(wm_h.at[:, half_in], wm.at[own + (core,)], wmx_s, wmx_r, partner)
    expect(wmx_s, wm.at[own + (0,)], wmx_s, wmx_r)
    for i, w in enumerate((wq_h, wf_h, wi_h, wo_h)):
        remote(w, wp.at[i, core], pw_s.at[i], pw_r.at[i], partner)
        expect((pw_s, i), wp.at[i, 0], pw_s.at[i], pw_r.at[i])
    c_small = [
        local(a, b, loc.at[6 + i])
        for i, (a, b) in enumerate(
            ((lb_h, lb), (hg_h, hg), (g1_h, g1), (b1_h, b1), (router_h, rt), (branch_h, br),
             (g2_h, g2), (b2_h, b2), (routes_h, rts))
        )
    ]
    c_st = [local(state_h.at[t], st.at[t], stsem.at[t]) for t in range(4)]
    c_w = []
    big = ((dg_h, dg), (du_h, du), (dd_h, dd), (eg_h, eg), (eu_h, eu), (ed_h, ed))
    for i, (a, b) in enumerate(big):
        c_w.append(local(a, b.at[core], loc.at[15 + i]))
    for part in range(3):
        walk_send(*of_tb, part, 1, tk_s, tk_r)
        walk_last(*of_tb, part, 0, tk_s, tk_r)
    c_wm.wait()
    got(wmx_s)
    for part in range(3):
        walk_send(*of_wm, part, 0, wm_s, wm_r)
    for g in (1, 3, 2):
        for part in range(3):
            walk_last(*of_tb, part, g, tk_s, tk_r)
    for part in range(3):
        walk_send(*of_wm, part, 1, wm_s, wm_r)
        walk_last(*of_wm, part, 0, wm_s, wm_r)
    for i, (a, b) in enumerate(big):
        remote(a, b.at[core], pw_s.at[4 + i], pw_r.at[4 + i], partner)
        expect((pw_s, 4 + i), b.at[0], pw_s.at[4 + i], pw_r.at[4 + i])

    for c in c_small:
        c.wait()
    expert = chip // 8
    r0 = rts[0:1, :]
    r1 = rts[1:2, :]
    lane = iota((1, 512), 1)
    hit = jnp.where((r0 == expert) | (r1 == expert), 1.0, 0.0)
    other = jnp.where(r0 == expert, r1, r0).astype(F32)
    mine = (lane // 4) % 2 == core

    def own_rows(v):
        moved = jnp.where(core == 0, pltpu.roll(v, 4, 1), pltpu.roll(v, 508, 1))
        return jnp.where(mine, v, moved)

    hit = own_rows(hit)
    other = own_rows(other)
    rank = jnp.zeros_like(hit)
    for d in range(1, 4):
        rank = rank + jnp.where(lane % 4 >= d, pltpu.roll(hit, d, 1), 0.0)
    srow, slane = iota((128, 256), 0), iota((128, 256), 1)
    fits = (srow // 64 == (slane // 4) % 2) & ((srow % 64) // 2 == slane // 8)
    sels, spreads = [], []
    for u in range(2):
        cols = slice(256 * u, 256 * (u + 1))
        sel = jnp.where(
            fits & (rank[:, cols] == (srow % 2).astype(F32)), jnp.broadcast_to(hit[:, cols], (128, 256)), 0.0
        )
        sels.append(sel.astype(BF16))
        spreads.append(jnp.transpose(sel).astype(BF16))
    other_t = jnp.transpose(jnp.broadcast_to(other, (128, 512)))
    wl = iota((512, 128), 1)
    pick = jnp.where(wl == 96 + expert, 1.0, 0.0) - jnp.where(wl == 96 + other_t.astype(jnp.int32), 1.0, 0.0)
    e_row, e_col = iota((128, 512), 0), iota((128, 512), 1)
    spread_e = jnp.where((e_row // 16 == e_col // 128) & (e_row % 16 == e_col % 16), 1.0, 0.0).astype(BF16)
    m_row, m_col = iota((512, 512), 0), iota((512, 512), 1)
    in_place = (m_row // 8) % 8 == (m_col // 16) % 8
    s_row, s_col = iota((32, 512), 0), iota((32, 512), 1)
    fold = jnp.where((s_col // 64 == s_row % 8) & (s_col % 8 == s_row // 8), 1.0, 0.0).astype(BF16)

    for i in range(4):
        c_wp[i].wait()
        got((pw_s, i))
    w64 = wp.reshape(64, 2048)
    w128 = jnp.concatenate([w64[:, :HALF], w64[:, HALF:]], axis=0)
    for part in range(3):
        got((tk_s, part, 4))
    proj = dot_nt(tb.reshape(512, HALF)[...], w128)
    proj = proj + pltpu.roll(pltpu.roll(proj, 508, 0), 64, 1)
    msg.reshape(512, 128)[...] = proj.astype(BF16)

    @pl.loop(1, 64)
    def _(j):
        to = (chip + j) % 64
        remote(msg.at[to], rcv.at[chip], a2_s, a2_r, 2 * to + core)

    expect(a2_s, rcv.at[0:63], a2_s, a2_r)
    rcv[chip] = msg[chip]
    for g in (1, 3, 2):
        for part in range(3):
            walk_last(*of_wm, part, g, wm_s, wm_r)

    wd[...] = jnp.zeros_like(wd)
    wdd[...] = jnp.zeros_like(wdd)
    for i in range(6):
        c_w[i].wait()
        got((pw_s, 4 + i))
    for c in range(2):
        for h in range(2):
            ls = slice(HALF * h, HALF * (h + 1))
            wd[256 * h + 48 * c : 256 * h + 48 * c + 44, :] = dg[c, :, ls]
            wd[256 * h + 128 + 48 * c : 256 * h + 128 + 48 * c + 44, :] = du[c, :, ls]
            wdd[128 * h + 48 * c : 128 * h + 48 * c + 44, :] = dd[c, :, ls]
    for h in range(2):
        ls = slice(HALF * h, HALF * (h + 1))
        brow = jnp.concatenate([br[8 * h + i : 8 * h + i + 1, :].astype(F32) for i in range(8)], axis=1)
        extra = jnp.concatenate([rt[:, ls].astype(F32), brow, jnp.zeros((7, HALF), F32)], axis=0)
        wd[256 * h + 96 : 256 * h + 112, :] = extra.astype(BF16)

    got(a2_s)
    wide = dot(rcv.reshape(512, 128)[...], spread_e)
    wide = jnp.where(in_place, wide, 0.0).astype(BF16)
    rows = dot(fold, wide)
    query, f_in, value, outgate = (rows[:, 128 * i : 128 * (i + 1)] for i in range(4))
    low = jnp.concatenate([lb[...]] * 4, axis=0)
    forget = low + (1.0 - low) * sigmoid(f_in)
    keyed = (1.0 - low) * sigmoid(-f_in)
    cols = jnp.transpose(jnp.concatenate([forget, keyed, query, query], axis=0))
    c_out = []
    for t in range(4):
        c_st[t].wait()
        for h in range(8):
            r = 8 * t + h
            fresh = cols[:, r : r + 1] * st[t, h] + cols[:, 32 + r : 33 + r] * value[r : r + 1, :]
            nst[t, h] = fresh
            rd[r : r + 1, :] = jnp.sum(fresh * cols[:, 64 + r : 65 + r], axis=0, keepdims=True)
        c_out.append(local(nst.at[t], nst_h.at[t], nsem.at[t]))
    read = rd[...]
    scaled = read * lax.rsqrt(jnp.mean(read * read, axis=1, keepdims=True) + HEAD_EPS) * hg[...]
    mx[core] = (scaled * (outgate * sigmoid(outgate))).astype(BF16).astype(F32)
    remote(mx.at[core], mx.at[core], mx_s.at[0], mx_r.at[0], partner)
    expect((mx_s, 0), mx.at[0], mx_s.at[0], mx_r.at[0])
    for part in range(3):
        got((wm_s, part, 4))
    got((mx_s, 0))
    mxv = mx.reshape(64, 128)
    lhs = jnp.concatenate([mxv[pl.ds(4 * core + i, 8, stride=8), :] for i in range(4)], axis=1).astype(BF16)
    mo = dot_nt(lhs, wm.reshape(2048, 512)[...])
    mos[0] = mo[:4]
    mos[1] = mo[4:]
    remote(mos.at[1 - core], mor, mx_s.at[1], mx_r.at[1], partner)
    expect((mx_s, 1), mor, mx_s.at[1], mx_r.at[1])
    mo = mos[core]
    got((mx_s, 1))
    mo = (mo + mor[...]).astype(BF16).astype(F32)
    pre = ALPHA * toks + mo
    center = jnp.mean(pre, axis=1, keepdims=True)
    var = jnp.mean(jnp.square(pre - center), axis=1, keepdims=True)
    normed = ((pre - center) * lax.rsqrt(var + NORM_EPS) * g1[...] + b1[...]).astype(BF16).astype(F32)
    nblk = jnp.concatenate([normed[:, :HALF], normed[:, HALF:]], axis=0)
    nb[own] = nblk.astype(BF16)

    for part in range(3):
        plane_send(nb, part, nb_s, nb_r)
    for g in (0, 1, 3, 2):
        for part in range(3):
            line_send(nb, part, g, nb_s, nb_r)
    for part in range(3):
        got((nb_s, part, 4))

    nbv = nb.reshape(512, HALF)
    for u in range(2):
        sel = dot(sels[u], nbv[256 * u : 256 * (u + 1), :]).astype(BF16)
        xe[64 * u : 64 * (u + 1), :HALF] = sel[:64]
        xe[64 * u : 64 * (u + 1), HALF:] = sel[64:]
    gate = dot_nt(xe[...], eg.reshape(896, 2048)[...])
    up = dot_nt(xe[...], eu.reshape(896, 2048)[...])
    hidden = (gate * sigmoid(gate) * up).astype(BF16)
    y2 = dot_nt(nbv[...], wd[...])
    first_half = (iota((512, 256), 0) // 4) % 2 == 0
    y = jnp.where(first_half, y2[:, :256], y2[:, 256:]).reshape(64, 8, 256)
    y = (y + pltpu.roll(y, 4, 1)).reshape(512, 256)
    yg = y[:, :128]
    weight = sigmoid(jnp.sum(yg * pick, axis=1, keepdims=True))
    branch = sigmoid(yg[:, 104:105])
    hd = yg * sigmoid(yg) * y[:, 128:] * branch
    top = (iota((512, 128), 0) // 4) % 2 == 0
    hdd = jnp.concatenate([jnp.where(top, hd, 0.0), jnp.where(top, 0.0, hd)], axis=1).astype(BF16)
    slots = dot(hidden, ed.reshape(896, 2048)[...]).astype(BF16)
    obv = ob.reshape(512, HALF)
    for u in range(2):
        ru = slice(256 * u, 256 * (u + 1))
        rows_u = jnp.concatenate([slots[64 * u : 64 * (u + 1), :HALF], slots[64 * u : 64 * (u + 1), HALF:]], axis=0)
        total = weight[ru] * dot(spreads[u], rows_u) + dot(hdd[ru], wdd[...])
        obv[ru, :] = total.astype(BF16)

    r1s, r2s, t1s = (r1a, r1b, r1c), (r2a, r2b, r2c), (t1a, t1b, t1c)
    spots = ((2, 0), (1, 1), (3, 2), (0, 3))
    for g, slot in spots:
        for part in range(3):
            d1, d2, _ = ORDERS[part]
            for k in (2, 1, 3):
                idx = region(part, {d1: (at[d1] + k) % 4, d2: (at[d2] + g) % 4})
                remote(
                    ob.at[idx + TAILS[part]], r1s[part].at[slot, k - 1], rs_s.at[part, slot], rs_r.at[part, slot],
                    peer({d1: k}),
                )
            expect((rs_s, part, slot), r1s[part].at[slot], rs_s.at[part, slot], rs_r.at[part, slot])
    for g, slot in spots:
        for part in range(3):
            d1, d2, d3 = ORDERS[part]
            got((rs_s, part, slot))
            idx = region(part, {d1: at[d1], d2: (at[d2] + g) % 4})
            total = ob[idx + TAILS[part]].astype(F32)
            for k in range(3):
                total = total + r1s[part][slot, k].astype(F32)
            t1s[part][slot] = total.astype(BF16)
            for k in (2, 1, 3, 0):
                if k or g:
                    remote(
                        t1s[part].at[slot, (at[d3] + k) % 4], r2s[part].at[4 * g + k - 1], rs_s.at[part, 4],
                        rs_r.at[part, 4], peer({d2: g, d3: k}),
                    )
    chans = []
    for part in range(3):
        d3 = ORDERS[part][2]
        take(r2s[part], rs_r.at[part, 4])
        total = t1s[part][3, at[d3]].astype(F32)
        for k in range(15):
            total = total + r2s[part][k].astype(F32)
        chans.append(total)
        sent[f"r{part}"] = functools.partial(take, r2s[part], rs_s.at[part, 4])
    z = ALPHA * nblk + jnp.concatenate(chans, axis=1)

    def both(v):
        v = jnp.broadcast_to(v, (8, 128))
        return (v + pltpu.roll(v, 4, 0))[:, 0:1]

    def by_half(ref):
        v = ref[...]
        return jnp.concatenate(
            [jnp.broadcast_to(v[:, :HALF], (4, HALF)), jnp.broadcast_to(v[:, HALF:], (4, HALF))], axis=0
        )

    center = both(jnp.sum(z, axis=1, keepdims=True)) * (1.0 / 2048)
    dev = z - center
    var = both(jnp.sum(dev * dev, axis=1, keepdims=True)) * (1.0 / 2048)
    res = dev * lax.rsqrt(var + NORM_EPS) * by_half(g2) + by_half(b2)
    outv[:, :HALF] = res[:4].astype(BF16)
    outv[:, HALF:] = res[4:].astype(BF16)
    c_out.append(local(outv, out_h, loc.at[0]))

    for c in c_out:
        c.wait()
    for wait in sent.values():
        wait()


def closing(a_h, s_h, out_h, nst_h, av, sv, into, out):
    ins = [pltpu.make_async_copy(s_h.at[t], sv.at[t], into.at[t]) for t in range(4)]
    ins.append(pltpu.make_async_copy(a_h, av, into.at[4]))
    outs = [pltpu.make_async_copy(sv.at[t], nst_h.at[t], out.at[t]) for t in range(4)]
    outs.append(pltpu.make_async_copy(av, out_h, out.at[4]))
    for cp in ins:
        cp.start()
    for cp, back in zip(ins, outs):
        cp.wait()
        back.start()
    for back in outs:
        back.wait()


def per_device(
    tokens, recurrent_state, query_weight, forget_weight, input_weight, outgate_weight, lower_bound, head_gain,
    mixout_weight, first_gain, first_bias, router_weight, branch_vector, dense_gate_weight, dense_up_weight,
    dense_down_weight, expert_gate_weight, expert_up_weight, expert_down_weight, second_gain, second_bias, routes,
):
    args = (
        tokens, recurrent_state, query_weight.T, forget_weight.T, input_weight.T, outgate_weight.T,
        lower_bound.reshape(8, 128), head_gain.reshape(1, 128), mixout_weight.T, first_gain.reshape(1, 2048),
        first_bias.reshape(1, 2048), router_weight.T, branch_vector.reshape(16, 128), dense_gate_weight.T,
        dense_up_weight.T, dense_down_weight, expert_gate_weight.T, expert_up_weight.T, expert_down_weight,
        second_gain.reshape(1, 2048), second_bias.reshape(1, 2048), routes.T,
    )
    lanes = [p.stop - p.start for p in LANES]
    V = pltpu.VMEM
    sem = pltpu.SemaphoreType.DMA
    scratch = [
        V((4, 2048), BF16), V((4, 2048), BF16), V((4, 8, 128, 128), F32), V((4, 8, 128, 128), F32), V((4, 2, 8, 2048), BF16),
        V((8, 128), F32), V((1, 128), F32), V((4, 4, 4, 2, 16, 512), BF16), V((1, 2048), F32), V((1, 2048), F32),
        V((8, 2048), BF16), V((16, 128), BF16), V((2, 44, 2048), BF16), V((2, 44, 2048), BF16),
        V((2, 44, 2048), BF16), V((2, 448, 2048), BF16), V((2, 448, 2048), BF16), V((2, 448, 2048), BF16),
        V((1, 2048), F32), V((1, 2048), F32), V((2, 512), jnp.int32),
        V((4, 4, 4, 8, HALF), BF16), V((4, 4, 4, 8, HALF), BF16), V((64, 8, 128), BF16), V((64, 8, 128), BF16),
        V((4, 4, 4, 8, HALF), BF16), V((128, 2048), BF16), V((512, HALF), BF16), V((256, HALF), BF16),
        V((32, 128), F32),
        *[V((4, 3, 4, 8, n), BF16) for n in lanes], *[V((15, 8, n), BF16) for n in lanes],
        *[V((4, 4, 8, n), BF16) for n in lanes],
        V((2, 32, 128), F32), V((2, 4, 2048), F32), V((4, 2048), F32),
        sem((21,)), sem((4,)), sem((4,)), sem((10,)), sem((10,)), sem((3, 5)), sem((3, 5)), sem(()), sem(()),
        sem((2,)), sem((2,)), sem((3, 5)), sem((3, 5)), sem((3, 5)), sem((3, 5)), sem(()), sem(()), sem((3, 5)), sem((3, 5)),
    ]
    hbm = pl.BlockSpec(memory_space=pltpu.HBM)
    free = pl.BlockSpec(memory_space=pl.ANY)
    shapes = (jax.ShapeDtypeStruct((4, 2048), BF16), jax.ShapeDtypeStruct((4, 8, 128, 128), F32))
    res = pl.pallas_call(
        kernel,
        out_shape=shapes,
        in_specs=[hbm] * 22,
        out_specs=(free, free),
        scratch_shapes=scratch,
        compiler_params=pltpu.CompilerParams(
            collective_id=0, has_side_effects=True, vmem_limit_bytes=60 * 1024 * 1024
        ),
        name="layer",
    )(*args)
    return pl.pallas_call(
        closing,
        out_shape=shapes,
        in_specs=[free] * 2,
        out_specs=(free, free),
        scratch_shapes=[V((4, 2048), BF16), V((4, 8, 128, 128), F32), sem((5,)), sem((5,))],
        compiler_params=pltpu.CompilerParams(vmem_limit_bytes=60 * 1024 * 1024),
        name="closing",
    )(*res)


def solution(mesh):
    ep = "ep"
    cols, rows = P(None, ep), P(ep, None)
    return jax.shard_map(
        per_device,
        mesh=mesh,
        in_specs=(
            rows, P(ep, None, None, None), cols, cols, cols, cols, P(), P(), cols, P(), P(), P(), P(),
            cols, cols, rows, cols, cols, rows, P(), P(), P(),
        ),
        out_specs=(rows, P(ep, None, None, None)),
        check_vma=False,
    )
```

```python
import functools

import jax
import jax.numpy as jnp
from jax import lax
from jax.experimental import pallas as pl
from jax.experimental.pallas import tpu as pltpu
from jax.sharding import PartitionSpec as P

ALPHA = 8.0**0.25
NORM_EPS = 1e-05
HEAD_EPS = 1e-06
HALF = 1024
F32 = jnp.float32
BF16 = jnp.bfloat16
ALL = slice(None)
ORDERS = ((2, 1, 0), (1, 0, 2), (0, 2, 1))
LANES = (slice(0, 384), slice(384, 768), slice(768, 1024))
TAILS = tuple((ALL, lanes) for lanes in LANES)
WTAILS = ((ALL, slice(0, 8), slice(0, 384)), (ALL, slice(8, 16), slice(0, 384)), (ALL, ALL, slice(384, 512)))
NT = (((1,), (1,)), ((), ()))


def dot(a, b):
    return jnp.dot(a, b, preferred_element_type=F32)


def dot_nt(a, b):
    return lax.dot_general(a, b, NT, preferred_element_type=F32)


def iota(shape, dim):
    return lax.broadcasted_iota(jnp.int32, shape, dim)


def id_of(part):
    return part if isinstance(part, int) else id(part)


def sigmoid(a):
    return 1.0 / (1.0 + jnp.exp(-a))


def kernel(
    tok_h, state_h, wq_h, wf_h, wi_h, wo_h, lb_h, hg_h, wm_h, g1_h, b1_h, router_h, branch_h,
    dg_h, du_h, dd_h, eg_h, eu_h, ed_h, g2_h, b2_h, routes_h,
    out_h, nst_h,
    tokv, outv, st, nst, wp, lb, hg, wm, g1, b1, rt, br, dg, du, dd, eg, eu, ed, g2, b2, rts,
    tb, nb, msg, rcv, ob, xe, wd, wdd, rd,
    r1a, r1b, r1c, r2a, r2b, r2c, t1a, t1b, t1c, mx, mos, mor, egt, eut,
    loc, stsem, nsem, pw_s, pw_r, wm_s, wm_r, wmx_s, wmx_r, mx_s, mx_r, tk_s, tk_r, nb_s, nb_r, a2_s, a2_r, rs_s, rs_r,
):
    me = lax.axis_index("ep")
    core = me % 2
    chip = me // 2
    at = (chip // 16, (chip // 4) % 4, chip % 4)
    partner = me + 1 - 2 * core

    def peer(steps):
        c = [(at[d] + steps[d]) % 4 if steps.get(d) else at[d] for d in range(3)]
        return 2 * ((c[0] * 4 + c[1]) * 4 + c[2]) + core

    def remote(src, dst, ss, rs, dev):
        pltpu.make_async_remote_copy(
            src_ref=src, dst_ref=dst, send_sem=ss, recv_sem=rs, device_id=(dev,),
            device_id_type=pl.DeviceIdType.MESH,
        ).start()

    sent, due = {}, {}

    def local(src, dst, sem):
        cp = pltpu.make_async_copy(src, dst, sem)
        cp.start()
        return cp

    def expect(key, ref, ss, rs):
        key = tuple(map(id_of, key)) if isinstance(key, tuple) else id_of(key)
        sent[key] = functools.partial(take, ref, ss)
        due[key] = functools.partial(take, ref, rs)

    def got(key):
        key = tuple(map(id_of, key)) if isinstance(key, tuple) else id_of(key)
        due.pop(key)()

    def take(ref, sem):
        pltpu.make_async_copy(ref, ref, sem).wait()

    own = (at[0], at[1], at[2])
    four = pl.ds(0, 4)
    rcv[...] = jnp.zeros_like(rcv)
    barrier = pltpu.get_barrier_semaphore()
    for step in [{d: k} for d in range(3) for k in (2, 1, 3)]:
        pl.semaphore_signal(barrier, inc=1, device_id=(peer(step),), device_id_type=pl.DeviceIdType.MESH)
    pl.semaphore_signal(barrier, inc=1, device_id=(partner,), device_id_type=pl.DeviceIdType.MESH)
    c_tok = local(tok_h, tokv, loc.at[0])
    half_own = pl.ds(pl.multiple_of(core * 512, 512), 512)
    c_wm = local(wm_h.at[:, half_own], wm.at[own + (core,)], loc.at[5])
    c_wp = [local(w, wp.at[i, core], loc.at[1 + i]) for i, w in enumerate((wq_h, wf_h, wi_h, wo_h))]
    c_tok.wait()
    toks = tokv[...].astype(F32)
    tblk = jnp.concatenate([toks[:, :HALF], toks[:, HALF:]], axis=0).astype(BF16)
    tb[own] = tblk
    pl.semaphore_wait(barrier, 10)

    def region(part, fixed):
        return tuple(fixed.get(d, ALL) for d in range(3))

    def blocks(buf, tail, count):
        idx = {3: (0, 0, slice(0, 3)), 4: (0, 0, ALL), 12: (0, slice(0, 3), ALL), 48: (slice(0, 3), ALL, ALL)}[count]
        return buf.at[idx + tail]

    def plane_send(buf, part, ss, rs):
        d1, d2, _ = ORDERS[part]
        ref = buf.at[own + TAILS[part]]
        for k2 in (0, 1, 3, 2):
            for k1 in (1, 3, 2, 0):
                if k1 or k2:
                    remote(ref, ref, ss.at[part, k2], rs.at[part, (4 - k2) % 4], peer({d1: k1, d2: k2}))
        for g in range(4):
            expect((ss, part, g), blocks(buf, TAILS[part], 4 if g else 3), ss.at[part, g], rs.at[part, g])

    def line_send(buf, part, g, ss, rs):
        d1, d2, d3 = ORDERS[part]
        got((ss, part, g))
        idx = region(part, {d2: (at[d2] + g) % 4, d3: at[d3]})
        ref = buf.at[idx + TAILS[part]]
        for k in (2, 1, 3):
            remote(ref, ref, ss.at[part, 4], rs.at[part, 4], peer({d3: k}))
        if g == 2:
            expect((ss, part, 4), blocks(buf, TAILS[part], 48), ss.at[part, 4], rs.at[part, 4])

    def walk_send(buf, tails, part, phase, ss, rs):
        d1, d2, d3 = ORDERS[part]
        if phase:
            got((ss, part, 0))
        ref = buf.at[region(part, {d: at[d] for d in (d1, d2, d3)[phase:]}) + tails[part]]
        for k in (2, 1, 3):
            sems = (0, 0) if phase == 0 else (k, 4 - k)
            remote(ref, ref, ss.at[part, sems[0]], rs.at[part, sems[1]], peer({(d1, d2)[phase]: k}))
        for g in range(1, 4) if phase else (0,):
            expect((ss, part, g), blocks(buf, tails[part], 4 if phase else 3), ss.at[part, g], rs.at[part, g])

    def walk_last(buf, tails, part, g, ss, rs):
        _, d2, d3 = ORDERS[part]
        if g:
            got((ss, part, g))
        ref = buf.at[region(part, {d2: (at[d2] + g) % 4, d3: at[d3]}) + tails[part]]
        for k in (2, 1, 3):
            remote(ref, ref, ss.at[part, 4], rs.at[part, 4], peer({d3: k}))
        if g == 2:
            expect((ss, part, 4), blocks(buf, tails[part], 48), ss.at[part, 4], rs.at[part, 4])

    of_wm, of_tb = (wm, WTAILS), (tb, TAILS)
    for part in range(3):
        walk_send(*of_tb, part, 0, tk_s, tk_r)
    half_in = pl.ds(pl.multiple_of((1 - core) * 512, 512), 512)
    remote(wm_h.at[:, half_in], wm.at[own + (core,)], wmx_s, wmx_r, partner)
    expect(wmx_s, wm.at[own + (0,)], wmx_s, wmx_r)
    for i, w in enumerate((wq_h, wf_h, wi_h, wo_h)):
        remote(w, wp.at[i, core], pw_s.at[i], pw_r.at[i], partner)
        expect((pw_s, i), wp.at[i, 0], pw_s.at[i], pw_r.at[i])
    c_small = [
        local(a, b, loc.at[6 + i])
        for i, (a, b) in enumerate(
            ((lb_h, lb), (hg_h, hg), (g1_h, g1), (b1_h, b1), (router_h, rt), (branch_h, br),
             (g2_h, g2), (b2_h, b2), (routes_h, rts))
        )
    ]
    c_st = [local(state_h.at[t], st.at[t], stsem.at[t]) for t in range(4)]
    c_w = []
    big = ((dg_h, dg), (du_h, du), (dd_h, dd), (eg_h, eg), (eu_h, eu), (ed_h, ed))
    for i, (a, b) in enumerate(big):
        c_w.append(local(a, b.at[core], loc.at[15 + i]))
    c_wm.wait()
    got(wmx_s)
    for part in range(3):
        walk_send(*of_wm, part, 0, wm_s, wm_r)
    for part in range(3):
        walk_send(*of_tb, part, 1, tk_s, tk_r)
        walk_last(*of_tb, part, 0, tk_s, tk_r)
    for g in (1, 3, 2):
        for part in range(3):
            walk_last(*of_tb, part, g, tk_s, tk_r)
    for part in range(3):
        walk_send(*of_wm, part, 1, wm_s, wm_r)
        walk_last(*of_wm, part, 0, wm_s, wm_r)
    for i, (a, b) in enumerate(big):
        remote(a, b.at[core], pw_s.at[4 + i], pw_r.at[4 + i], partner)
        expect((pw_s, 4 + i), b.at[0], pw_s.at[4 + i], pw_r.at[4 + i])

    for c in c_small:
        c.wait()
    expert = chip // 8
    r0 = rts[0:1, :]
    r1 = rts[1:2, :]
    lane = iota((1, 512), 1)
    hit = jnp.where((r0 == expert) | (r1 == expert), 1.0, 0.0)
    other = jnp.where(r0 == expert, r1, r0).astype(F32)
    mine = (lane // 4) % 2 == core

    def own_rows(v):
        moved = jnp.where(core == 0, pltpu.roll(v, 4, 1), pltpu.roll(v, 508, 1))
        return jnp.where(mine, v, moved)

    hit = own_rows(hit)
    other = own_rows(other)
    rank = jnp.zeros_like(hit)
    for d in range(1, 4):
        rank = rank + jnp.where(lane % 4 >= d, pltpu.roll(hit, d, 1), 0.0)
    srow, slane = iota((128, 256), 0), iota((128, 256), 1)
    fits = (srow // 64 == (slane // 4) % 2) & ((srow % 64) // 2 == slane // 8)
    sels, spreads = [], []
    for u in range(2):
        cols = slice(256 * u, 256 * (u + 1))
        sel = jnp.where(
            fits & (rank[:, cols] == (srow % 2).astype(F32)), jnp.broadcast_to(hit[:, cols], (128, 256)), 0.0
        )
        sels.append(sel.astype(BF16))
        spreads.append(jnp.transpose(sel).astype(BF16))
    other_t = jnp.transpose(jnp.broadcast_to(other, (128, 512)))
    wl = iota((512, 128), 1)
    pick = jnp.where(wl == 96 + expert, 1.0, 0.0) - jnp.where(wl == 96 + other_t.astype(jnp.int32), 1.0, 0.0)
    e_row, e_col = iota((128, 512), 0), iota((128, 512), 1)
    spread_e = jnp.where((e_row // 16 == e_col // 128) & (e_row % 16 == e_col % 16), 1.0, 0.0).astype(BF16)
    m_row, m_col = iota((512, 512), 0), iota((512, 512), 1)
    in_place = (m_row // 8) % 8 == (m_col // 16) % 8
    s_row, s_col = iota((32, 512), 0), iota((32, 512), 1)
    fold = jnp.where((s_col // 64 == s_row % 8) & (s_col % 8 == s_row // 8), 1.0, 0.0).astype(BF16)

    def turn(c):
        egt[c] = jnp.transpose(eg[c])
        eut[c] = jnp.transpose(eu[c])

    for i in range(6):
        c_w[i].wait()
    turn(core)
    for i in range(4):
        c_wp[i].wait()
        got((pw_s, i))
    w64 = wp.reshape(64, 2048)
    w128 = jnp.concatenate([w64[:, :HALF], w64[:, HALF:]], axis=0)
    for part in range(3):
        got((tk_s, part, 4))
    proj = dot_nt(tb.reshape(512, HALF)[...], w128)
    proj = proj + pltpu.roll(pltpu.roll(proj, 508, 0), 64, 1)
    msg.reshape(512, 128)[...] = proj.astype(BF16)

    @pl.loop(1, 64)
    def _(j):
        to = (chip + j) % 64
        remote(msg.at[to, four], rcv.at[chip, four], a2_s, a2_r, 2 * to + core)

    expect(a2_s, rcv.at[0:63, four], a2_s, a2_r)
    rcv[chip, four] = msg[chip, four]
    for g in (1, 3, 2):
        for part in range(3):
            walk_last(*of_wm, part, g, wm_s, wm_r)

    wd[...] = jnp.zeros_like(wd)
    wdd[...] = jnp.zeros_like(wdd)
    for i in range(6):
        got((pw_s, 4 + i))
    for c in range(2):
        for h in range(2):
            ls = slice(HALF * h, HALF * (h + 1))
            wd[256 * h + 48 * c : 256 * h + 48 * c + 44, :] = dg[c, :, ls]
            wd[256 * h + 128 + 48 * c : 256 * h + 128 + 48 * c + 44, :] = du[c, :, ls]
            wdd[128 * h + 48 * c : 128 * h + 48 * c + 44, :] = dd[c, :, ls]
    for h in range(2):
        ls = slice(HALF * h, HALF * (h + 1))
        brow = jnp.concatenate([br[8 * h + i : 8 * h + i + 1, :].astype(F32) for i in range(8)], axis=1)
        extra = jnp.concatenate([rt[:, ls].astype(F32), brow, jnp.zeros((7, HALF), F32)], axis=0)
        wd[256 * h + 96 : 256 * h + 112, :] = extra.astype(BF16)

    got(a2_s)
    wide = dot(rcv.reshape(512, 128)[...], spread_e)
    wide = jnp.where(in_place, wide, 0.0).astype(BF16)
    rows = dot(fold, wide)
    query, f_in, value, outgate = (rows[:, 128 * i : 128 * (i + 1)] for i in range(4))
    low = jnp.concatenate([lb[...]] * 4, axis=0)
    forget = low + (1.0 - low) * sigmoid(f_in)
    keyed = (1.0 - low) * sigmoid(-f_in)
    cols = jnp.transpose(jnp.concatenate([forget, keyed, query, query], axis=0))
    c_out = []
    for t in range(4):
        c_st[t].wait()
        for h in range(8):
            r = 8 * t + h
            fresh = cols[:, r : r + 1] * st[t, h] + cols[:, 32 + r : 33 + r] * value[r : r + 1, :]
            nst[t, h] = fresh
            rd[r : r + 1, :] = jnp.sum(fresh * cols[:, 64 + r : 65 + r], axis=0, keepdims=True)
        c_out.append(local(nst.at[t], nst_h.at[t], nsem.at[t]))
    read = rd[...]
    scaled = read * lax.rsqrt(jnp.mean(read * read, axis=1, keepdims=True) + HEAD_EPS) * hg[...]
    mx[core] = (scaled * (outgate * sigmoid(outgate))).astype(BF16).astype(F32)
    remote(mx.at[core], mx.at[core], mx_s.at[0], mx_r.at[0], partner)
    expect((mx_s, 0), mx.at[0], mx_s.at[0], mx_r.at[0])
    for part in range(3):
        got((wm_s, part, 4))
    got((mx_s, 0))
    mxv = mx.reshape(64, 128)
    lhs = jnp.concatenate([mxv[pl.ds(4 * core + i, 8, stride=8), :] for i in range(4)], axis=1).astype(BF16)
    mo = dot_nt(lhs, wm.reshape(2048, 512)[...])
    mos[0] = mo[:4]
    mos[1] = mo[4:]
    remote(mos.at[1 - core], mor, mx_s.at[1], mx_r.at[1], partner)
    expect((mx_s, 1), mor, mx_s.at[1], mx_r.at[1])
    mo = mos[core]
    got((mx_s, 1))
    mo = (mo + mor[...]).astype(BF16).astype(F32)
    pre = ALPHA * toks + mo
    center = jnp.mean(pre, axis=1, keepdims=True)
    var = jnp.mean(jnp.square(pre - center), axis=1, keepdims=True)
    normed = ((pre - center) * lax.rsqrt(var + NORM_EPS) * g1[...] + b1[...]).astype(BF16).astype(F32)
    nblk = jnp.concatenate([normed[:, :HALF], normed[:, HALF:]], axis=0)
    nb[own] = nblk.astype(BF16)

    for part in range(3):
        plane_send(nb, part, nb_s, nb_r)
    turn(1 - core)
    for g in (0, 1, 3, 2):
        for part in range(3):
            line_send(nb, part, g, nb_s, nb_r)
    for part in range(3):
        got((nb_s, part, 4))

    nbv = nb.reshape(512, HALF)
    for u in range(2):
        sel = dot(sels[u], nbv[256 * u : 256 * (u + 1), :]).astype(BF16)
        xe[64 * u : 64 * (u + 1), :HALF] = sel[:64]
        xe[64 * u : 64 * (u + 1), HALF:] = sel[64:]
    xes = xe[...]
    hiddens = []
    for c in range(2):
        gate = dot(xes, egt[c])
        up = dot(xes, eut[c])
        hiddens.append((gate * sigmoid(gate) * up).astype(BF16))
    y2 = dot_nt(nbv[...], wd[...])
    first_half = (iota((512, 256), 0) // 4) % 2 == 0
    y = jnp.where(first_half, y2[:, :256], y2[:, 256:]).reshape(64, 8, 256)
    y = (y + pltpu.roll(y, 4, 1)).reshape(512, 256)
    yg = y[:, :128]
    weight = sigmoid(jnp.sum(yg * pick, axis=1, keepdims=True))
    branch = sigmoid(yg[:, 104:105])
    hd = yg * sigmoid(yg) * y[:, 128:] * branch
    top = (iota((512, 128), 0) // 4) % 2 == 0
    hdd = jnp.concatenate([jnp.where(top, hd, 0.0), jnp.where(top, 0.0, hd)], axis=1).astype(BF16)
    slots = (dot(hiddens[0], ed[0]) + dot(hiddens[1], ed[1])).astype(BF16)
    obv = ob.reshape(512, HALF)
    for u in range(2):
        ru = slice(256 * u, 256 * (u + 1))
        rows_u = jnp.concatenate([slots[64 * u : 64 * (u + 1), :HALF], slots[64 * u : 64 * (u + 1), HALF:]], axis=0)
        total = weight[ru] * dot(spreads[u], rows_u) + dot(hdd[ru], wdd[...])
        obv[ru, :] = total.astype(BF16)

    r1s, r2s, t1s = (r1a, r1b, r1c), (r2a, r2b, r2c), (t1a, t1b, t1c)
    spots = ((2, 0), (1, 1), (3, 2), (0, 3))
    for g, slot in spots:
        for part in range(3):
            d1, d2, _ = ORDERS[part]
            for k in (2, 1, 3):
                idx = region(part, {d1: (at[d1] + k) % 4, d2: (at[d2] + g) % 4})
                remote(
                    ob.at[idx + TAILS[part]], r1s[part].at[slot, k - 1], rs_s.at[part, slot], rs_r.at[part, slot],
                    peer({d1: k}),
                )
            expect((rs_s, part, slot), r1s[part].at[slot], rs_s.at[part, slot], rs_r.at[part, slot])
    for g, slot in spots:
        for part in range(3):
            d1, d2, d3 = ORDERS[part]
            got((rs_s, part, slot))
            idx = region(part, {d1: at[d1], d2: (at[d2] + g) % 4})
            total = ob[idx + TAILS[part]].astype(F32)
            for k in range(3):
                total = total + r1s[part][slot, k].astype(F32)
            t1s[part][slot] = total.astype(BF16)
            for k in (2, 1, 3, 0):
                if k or g:
                    remote(
                        t1s[part].at[slot, (at[d3] + k) % 4], r2s[part].at[4 * g + k - 1], rs_s.at[part, 4],
                        rs_r.at[part, 4], peer({d2: g, d3: k}),
                    )
    chans = []
    for part in range(3):
        d3 = ORDERS[part][2]
        take(r2s[part], rs_r.at[part, 4])
        total = t1s[part][3, at[d3]].astype(F32)
        for k in range(15):
            total = total + r2s[part][k].astype(F32)
        chans.append(total)
        sent[f"r{part}"] = functools.partial(take, r2s[part], rs_s.at[part, 4])
    z = ALPHA * nblk + jnp.concatenate(chans, axis=1)

    def both(v):
        v = jnp.broadcast_to(v, (8, 128))
        return (v + pltpu.roll(v, 4, 0))[:, 0:1]

    def by_half(ref):
        v = ref[...]
        return jnp.concatenate(
            [jnp.broadcast_to(v[:, :HALF], (4, HALF)), jnp.broadcast_to(v[:, HALF:], (4, HALF))], axis=0
        )

    center = both(jnp.sum(z, axis=1, keepdims=True)) * (1.0 / 2048)
    dev = z - center
    var = both(jnp.sum(dev * dev, axis=1, keepdims=True)) * (1.0 / 2048)
    res = dev * lax.rsqrt(var + NORM_EPS) * by_half(g2) + by_half(b2)
    outv[:, :HALF] = res[:4].astype(BF16)
    outv[:, HALF:] = res[4:].astype(BF16)
    c_out.append(local(outv, out_h, loc.at[0]))

    for c in c_out:
        c.wait()
    for wait in sent.values():
        wait()


def closing(a_h, s_h, out_h, nst_h, av, sv, into, out):
    ins = [pltpu.make_async_copy(s_h.at[t], sv.at[t], into.at[t]) for t in range(4)]
    ins.append(pltpu.make_async_copy(a_h, av, into.at[4]))
    outs = [pltpu.make_async_copy(sv.at[t], nst_h.at[t], out.at[t]) for t in range(4)]
    outs.append(pltpu.make_async_copy(av, out_h, out.at[4]))
    for cp in ins:
        cp.start()
    for cp, back in zip(ins, outs):
        cp.wait()
        back.start()
    for back in outs:
        back.wait()


def per_device(
    tokens, recurrent_state, query_weight, forget_weight, input_weight, outgate_weight, lower_bound, head_gain,
    mixout_weight, first_gain, first_bias, router_weight, branch_vector, dense_gate_weight, dense_up_weight,
    dense_down_weight, expert_gate_weight, expert_up_weight, expert_down_weight, second_gain, second_bias, routes,
):
    args = (
        tokens, recurrent_state, query_weight.T, forget_weight.T, input_weight.T, outgate_weight.T,
        lower_bound.reshape(8, 128), head_gain.reshape(1, 128), mixout_weight.T, first_gain.reshape(1, 2048),
        first_bias.reshape(1, 2048), router_weight.T, branch_vector.reshape(16, 128), dense_gate_weight.T,
        dense_up_weight.T, dense_down_weight, expert_gate_weight.T, expert_up_weight.T, expert_down_weight,
        second_gain.reshape(1, 2048), second_bias.reshape(1, 2048), routes.T,
    )
    lanes = [p.stop - p.start for p in LANES]
    V = pltpu.VMEM
    sem = pltpu.SemaphoreType.DMA
    scratch = [
        V((4, 2048), BF16), V((4, 2048), BF16), V((4, 8, 128, 128), F32), V((4, 8, 128, 128), F32), V((4, 2, 8, 2048), BF16),
        V((8, 128), F32), V((1, 128), F32), V((4, 4, 4, 2, 16, 512), BF16), V((1, 2048), F32), V((1, 2048), F32),
        V((8, 2048), BF16), V((16, 128), BF16), V((2, 44, 2048), BF16), V((2, 44, 2048), BF16),
        V((2, 44, 2048), BF16), V((2, 448, 2048), BF16), V((2, 448, 2048), BF16), V((2, 448, 2048), BF16),
        V((1, 2048), F32), V((1, 2048), F32), V((2, 512), jnp.int32),
        V((4, 4, 4, 8, HALF), BF16), V((4, 4, 4, 8, HALF), BF16), V((64, 8, 128), BF16), V((64, 8, 128), BF16),
        V((4, 4, 4, 8, HALF), BF16), V((128, 2048), BF16), V((512, HALF), BF16), V((256, HALF), BF16),
        V((32, 128), F32),
        *[V((4, 3, 4, 8, n), BF16) for n in lanes], *[V((15, 8, n), BF16) for n in lanes],
        *[V((4, 4, 8, n), BF16) for n in lanes],
        V((2, 32, 128), F32), V((2, 4, 2048), F32), V((4, 2048), F32), V((2, 2048, 448), BF16), V((2, 2048, 448), BF16),
        sem((21,)), sem((4,)), sem((4,)), sem((10,)), sem((10,)), sem((3, 5)), sem((3, 5)), sem(()), sem(()),
        sem((2,)), sem((2,)), sem((3, 5)), sem((3, 5)), sem((3, 5)), sem((3, 5)), sem(()), sem(()), sem((3, 5)), sem((3, 5)),
    ]
    hbm = pl.BlockSpec(memory_space=pltpu.HBM)
    free = pl.BlockSpec(memory_space=pl.ANY)
    shapes = (jax.ShapeDtypeStruct((4, 2048), BF16), jax.ShapeDtypeStruct((4, 8, 128, 128), F32))
    res = pl.pallas_call(
        kernel,
        out_shape=shapes,
        in_specs=[hbm] * 22,
        out_specs=(free, free),
        scratch_shapes=scratch,
        compiler_params=pltpu.CompilerParams(
            collective_id=0, has_side_effects=True, vmem_limit_bytes=60 * 1024 * 1024
        ),
        name="layer",
    )(*args)
    return pl.pallas_call(
        closing,
        out_shape=shapes,
        in_specs=[free] * 2,
        out_specs=(free, free),
        scratch_shapes=[V((4, 2048), BF16), V((4, 8, 128, 128), F32), sem((5,)), sem((5,))],
        compiler_params=pltpu.CompilerParams(vmem_limit_bytes=60 * 1024 * 1024),
        name="closing",
    )(*res)


def solution(mesh):
    ep = "ep"
    cols, rows = P(None, ep), P(ep, None)
    return jax.shard_map(
        per_device,
        mesh=mesh,
        in_specs=(
            rows, P(ep, None, None, None), cols, cols, cols, cols, P(), P(), cols, P(), P(), P(), P(),
            cols, cols, rows, cols, cols, rows, P(), P(), P(),
        ),
        out_specs=(rows, P(ep, None, None, None)),
        check_vma=False,
    )
```

```python
import functools

import jax
import jax.numpy as jnp
from jax import lax
from jax.experimental import pallas as pl
from jax.experimental.pallas import tpu as pltpu
from jax.sharding import PartitionSpec as P

ALPHA = 8.0**0.25
NORM_EPS = 1e-05
HEAD_EPS = 1e-06
HALF = 1024
F32 = jnp.float32
BF16 = jnp.bfloat16
ALL = slice(None)
ORDERS = ((2, 1, 0), (1, 0, 2), (0, 2, 1))
LANES = (slice(0, 384), slice(384, 768), slice(768, 1024))
TAILS = tuple((ALL, lanes) for lanes in LANES)
WTAILS = ((ALL, slice(0, 8), slice(0, 384)), (ALL, slice(8, 16), slice(0, 384)), (ALL, ALL, slice(384, 512)))
NT = (((1,), (1,)), ((), ()))


def dot(a, b):
    return jnp.dot(a, b, preferred_element_type=F32)


def dot_nt(a, b):
    return lax.dot_general(a, b, NT, preferred_element_type=F32)


def iota(shape, dim):
    return lax.broadcasted_iota(jnp.int32, shape, dim)


def id_of(part):
    return part if isinstance(part, int) else id(part)


def sigmoid(a):
    return 1.0 / (1.0 + jnp.exp(-a))


def kernel(
    tok_h, state_h, wq_h, wf_h, wi_h, wo_h, lb_h, hg_h, wm_h, g1_h, b1_h, router_h, branch_h,
    dg_h, du_h, dd_h, eg_h, eu_h, ed_h, g2_h, b2_h, routes_h,
    out_h, nst_h,
    tokv, outv, st, nst, wp, lb, hg, wm, g1, b1, rt, br, dg, du, dd, eg, eu, ed, g2, b2, rts,
    tb, nb, msg, rcv, ob, xe, wd, wdd, rd,
    r1a, r1b, r1c, r2a, r2b, r2c, t1a, t1b, t1c, mx, mos, mor, egt, eut,
    loc, stsem, nsem, pw_s, pw_r, wm_s, wm_r, wmx_s, wmx_r, mx_s, mx_r, tk_s, tk_r, nb_s, nb_r, a2_s, a2_r, rs_s, rs_r,
):
    me = lax.axis_index("ep")
    core = me % 2
    chip = me // 2
    at = (chip // 16, (chip // 4) % 4, chip % 4)
    partner = me + 1 - 2 * core

    def peer(steps):
        c = [(at[d] + steps[d]) % 4 if steps.get(d) else at[d] for d in range(3)]
        return 2 * ((c[0] * 4 + c[1]) * 4 + c[2]) + core

    def remote(src, dst, ss, rs, dev):
        pltpu.make_async_remote_copy(
            src_ref=src, dst_ref=dst, send_sem=ss, recv_sem=rs, device_id=(dev,),
            device_id_type=pl.DeviceIdType.MESH,
        ).start()

    sent, due = {}, {}

    def local(src, dst, sem):
        cp = pltpu.make_async_copy(src, dst, sem)
        cp.start()
        return cp

    def expect(key, ref, ss, rs):
        key = tuple(map(id_of, key)) if isinstance(key, tuple) else id_of(key)
        sent[key] = functools.partial(take, ref, ss)
        due[key] = functools.partial(take, ref, rs)

    def got(key):
        key = tuple(map(id_of, key)) if isinstance(key, tuple) else id_of(key)
        due.pop(key)()

    def take(ref, sem):
        pltpu.make_async_copy(ref, ref, sem).wait()

    own = (at[0], at[1], at[2])
    four = pl.ds(0, 4)
    rcv[...] = jnp.zeros_like(rcv)
    barrier = pltpu.get_barrier_semaphore()
    for step in [{d: k} for d in range(3) for k in (2, 1, 3)]:
        pl.semaphore_signal(barrier, inc=1, device_id=(peer(step),), device_id_type=pl.DeviceIdType.MESH)
    pl.semaphore_signal(barrier, inc=1, device_id=(partner,), device_id_type=pl.DeviceIdType.MESH)
    c_tok = local(tok_h, tokv, loc.at[0])
    half_own = pl.ds(pl.multiple_of(core * 512, 512), 512)
    c_wm = local(wm_h.at[:, half_own], wm.at[own + (core,)], loc.at[5])
    c_wp = [local(w, wp.at[i, core], loc.at[1 + i]) for i, w in enumerate((wq_h, wf_h, wi_h, wo_h))]
    c_tok.wait()
    toks = tokv[...].astype(F32)
    tblk = jnp.concatenate([toks[:, :HALF], toks[:, HALF:]], axis=0).astype(BF16)
    tb[own] = tblk
    pl.semaphore_wait(barrier, 10)

    def region(part, fixed):
        return tuple(fixed.get(d, ALL) for d in range(3))

    def blocks(buf, tail, count):
        idx = {3: (0, 0, slice(0, 3)), 4: (0, 0, ALL), 12: (0, slice(0, 3), ALL), 48: (slice(0, 3), ALL, ALL)}[count]
        return buf.at[idx + tail]

    def plane_send(buf, part, ss, rs):
        d1, d2, _ = ORDERS[part]
        ref = buf.at[own + TAILS[part]]
        for k2 in (0, 1, 3, 2):
            for k1 in (1, 3, 2, 0):
                if k1 or k2:
                    remote(ref, ref, ss.at[part, k2], rs.at[part, (4 - k2) % 4], peer({d1: k1, d2: k2}))
        for g in range(4):
            expect((ss, part, g), blocks(buf, TAILS[part], 4 if g else 3), ss.at[part, g], rs.at[part, g])

    def line_send(buf, part, g, ss, rs):
        d1, d2, d3 = ORDERS[part]
        got((ss, part, g))
        idx = region(part, {d2: (at[d2] + g) % 4, d3: at[d3]})
        ref = buf.at[idx + TAILS[part]]
        for k in (2, 1, 3):
            remote(ref, ref, ss.at[part, 4], rs.at[part, 4], peer({d3: k}))
        if g == 2:
            expect((ss, part, 4), blocks(buf, TAILS[part], 48), ss.at[part, 4], rs.at[part, 4])

    def walk_send(buf, tails, part, phase, ss, rs):
        d1, d2, d3 = ORDERS[part]
        if phase:
            got((ss, part, 0))
        ref = buf.at[region(part, {d: at[d] for d in (d1, d2, d3)[phase:]}) + tails[part]]
        for k in (2, 1, 3):
            sems = (0, 0) if phase == 0 else (k, 4 - k)
            remote(ref, ref, ss.at[part, sems[0]], rs.at[part, sems[1]], peer({(d1, d2)[phase]: k}))
        for g in range(1, 4) if phase else (0,):
            expect((ss, part, g), blocks(buf, tails[part], 4 if phase else 3), ss.at[part, g], rs.at[part, g])

    def walk_last(buf, tails, part, g, ss, rs):
        _, d2, d3 = ORDERS[part]
        if g:
            got((ss, part, g))
        ref = buf.at[region(part, {d2: (at[d2] + g) % 4, d3: at[d3]}) + tails[part]]
        for k in (2, 1, 3):
            remote(ref, ref, ss.at[part, 4], rs.at[part, 4], peer({d3: k}))
        if g == 2:
            expect((ss, part, 4), blocks(buf, tails[part], 48), ss.at[part, 4], rs.at[part, 4])

    of_wm, of_tb = (wm, WTAILS), (tb, TAILS)
    half_in = pl.ds(pl.multiple_of((1 - core) * 512, 512), 512)
    remote(wm_h.at[:, half_in], wm.at[own + (core,)], wmx_s, wmx_r, partner)
    expect(wmx_s, wm.at[own + (0,)], wmx_s, wmx_r)
    for part in range(3):
        walk_send(*of_tb, part, 0, tk_s, tk_r)
    for i, w in enumerate((wq_h, wf_h, wi_h, wo_h)):
        remote(w, wp.at[i, core], pw_s.at[i], pw_r.at[i], partner)
        expect((pw_s, i), wp.at[i, 0], pw_s.at[i], pw_r.at[i])
    c_small = [
        local(a, b, loc.at[6 + i])
        for i, (a, b) in enumerate(
            ((lb_h, lb), (hg_h, hg), (g1_h, g1), (b1_h, b1), (router_h, rt), (branch_h, br),
             (g2_h, g2), (b2_h, b2), (routes_h, rts))
        )
    ]
    c_st = [local(state_h.at[t], st.at[t], stsem.at[t]) for t in range(4)]
    c_w = []
    big = ((dg_h, dg), (du_h, du), (dd_h, dd), (eg_h, eg), (eu_h, eu), (ed_h, ed))
    for i, (a, b) in enumerate(big):
        c_w.append(local(a, b.at[core], loc.at[15 + i]))
    c_wm.wait()
    got(wmx_s)
    for part in range(3):
        walk_send(*of_wm, part, 0, wm_s, wm_r)
    for part in range(3):
        walk_send(*of_tb, part, 1, tk_s, tk_r)
        walk_last(*of_tb, part, 0, tk_s, tk_r)
    for g in (1, 3, 2):
        for part in range(3):
            walk_last(*of_tb, part, g, tk_s, tk_r)
    for part in range(3):
        walk_send(*of_wm, part, 1, wm_s, wm_r)
        walk_last(*of_wm, part, 0, wm_s, wm_r)
    for i, (a, b) in enumerate(big):
        remote(a, b.at[core], pw_s.at[4 + i], pw_r.at[4 + i], partner)
        expect((pw_s, 4 + i), b.at[0], pw_s.at[4 + i], pw_r.at[4 + i])

    for c in c_small:
        c.wait()
    expert = chip // 8
    r0 = rts[0:1, :]
    r1 = rts[1:2, :]
    lane = iota((1, 512), 1)
    hit = jnp.where((r0 == expert) | (r1 == expert), 1.0, 0.0)
    other = jnp.where(r0 == expert, r1, r0).astype(F32)
    mine = (lane // 4) % 2 == core

    def own_rows(v):
        moved = jnp.where(core == 0, pltpu.roll(v, 4, 1), pltpu.roll(v, 508, 1))
        return jnp.where(mine, v, moved)

    hit = own_rows(hit)
    other = own_rows(other)
    rank = jnp.zeros_like(hit)
    for d in range(1, 4):
        rank = rank + jnp.where(lane % 4 >= d, pltpu.roll(hit, d, 1), 0.0)
    srow, slane = iota((128, 256), 0), iota((128, 256), 1)
    fits = (srow // 64 == (slane // 4) % 2) & ((srow % 64) // 2 == slane // 8)
    sels, spreads = [], []
    for u in range(2):
        cols = slice(256 * u, 256 * (u + 1))
        sel = jnp.where(
            fits & (rank[:, cols] == (srow % 2).astype(F32)), jnp.broadcast_to(hit[:, cols], (128, 256)), 0.0
        )
        sels.append(sel.astype(BF16))
        spreads.append(jnp.transpose(sel).astype(BF16))
    other_t = jnp.transpose(jnp.broadcast_to(other, (128, 512)))
    wl = iota((512, 128), 1)
    pick = jnp.where(wl == 96 + expert, 1.0, 0.0) - jnp.where(wl == 96 + other_t.astype(jnp.int32), 1.0, 0.0)
    e_row, e_col = iota((128, 512), 0), iota((128, 512), 1)
    spread_e = jnp.where((e_row // 16 == e_col // 128) & (e_row % 16 == e_col % 16), 1.0, 0.0).astype(BF16)
    m_row, m_col = iota((512, 512), 0), iota((512, 512), 1)
    in_place = (m_row // 8) % 8 == (m_col // 16) % 8
    s_row, s_col = iota((32, 512), 0), iota((32, 512), 1)
    fold = jnp.where((s_col // 64 == s_row % 8) & (s_col % 8 == s_row // 8), 1.0, 0.0).astype(BF16)

    def turn(c):
        egt[c] = jnp.transpose(eg[c])
        eut[c] = jnp.transpose(eu[c])

    for i in range(6):
        c_w[i].wait()
    turn(core)
    for i in range(4):
        c_wp[i].wait()
        got((pw_s, i))
    w64 = wp.reshape(64, 2048)
    w128 = jnp.concatenate([w64[:, :HALF], w64[:, HALF:]], axis=0)
    for part in range(3):
        got((tk_s, part, 4))
    proj = dot_nt(tb.reshape(512, HALF)[...], w128)
    proj = proj + pltpu.roll(pltpu.roll(proj, 508, 0), 64, 1)
    msg.reshape(512, 128)[...] = proj.astype(BF16)

    @pl.loop(1, 64)
    def _(j):
        to = (chip + j) % 64
        remote(msg.at[to, four], rcv.at[chip, four], a2_s, a2_r, 2 * to + core)

    expect(a2_s, rcv.at[0:63, four], a2_s, a2_r)
    rcv[chip, four] = msg[chip, four]
    for g in (1, 3, 2):
        for part in range(3):
            walk_last(*of_wm, part, g, wm_s, wm_r)

    wd[...] = jnp.zeros_like(wd)
    wdd[...] = jnp.zeros_like(wdd)
    for i in range(3):
        got((pw_s, 4 + i))
    for c in range(2):
        for h in range(2):
            ls = slice(HALF * h, HALF * (h + 1))
            wd[256 * h + 48 * c : 256 * h + 48 * c + 44, :] = dg[c, :, ls]
            wd[256 * h + 128 + 48 * c : 256 * h + 128 + 48 * c + 44, :] = du[c, :, ls]
            wdd[128 * h + 48 * c : 128 * h + 48 * c + 44, :] = dd[c, :, ls]
    for h in range(2):
        ls = slice(HALF * h, HALF * (h + 1))
        brow = jnp.concatenate([br[8 * h + i : 8 * h + i + 1, :].astype(F32) for i in range(8)], axis=1)
        extra = jnp.concatenate([rt[:, ls].astype(F32), brow, jnp.zeros((7, HALF), F32)], axis=0)
        wd[256 * h + 96 : 256 * h + 112, :] = extra.astype(BF16)

    got(a2_s)
    wide = dot(rcv.reshape(512, 128)[...], spread_e)
    wide = jnp.where(in_place, wide, 0.0).astype(BF16)
    rows = dot(fold, wide)
    query, f_in, value, outgate = (rows[:, 128 * i : 128 * (i + 1)] for i in range(4))
    low = jnp.concatenate([lb[...]] * 4, axis=0)
    forget = low + (1.0 - low) * sigmoid(f_in)
    keyed = (1.0 - low) * sigmoid(-f_in)
    cols = jnp.transpose(jnp.concatenate([forget, keyed, query, query], axis=0))
    c_out = []
    for t in range(4):
        c_st[t].wait()
        for h in range(8):
            r = 8 * t + h
            fresh = cols[:, r : r + 1] * st[t, h] + cols[:, 32 + r : 33 + r] * value[r : r + 1, :]
            nst[t, h] = fresh
            rd[r : r + 1, :] = jnp.sum(fresh * cols[:, 64 + r : 65 + r], axis=0, keepdims=True)
        c_out.append(local(nst.at[t], nst_h.at[t], nsem.at[t]))
    read = rd[...]
    scaled = read * lax.rsqrt(jnp.mean(read * read, axis=1, keepdims=True) + HEAD_EPS) * hg[...]
    mx[core] = (scaled * (outgate * sigmoid(outgate))).astype(BF16).astype(F32)
    remote(mx.at[core], mx.at[core], mx_s.at[0], mx_r.at[0], partner)
    expect((mx_s, 0), mx.at[0], mx_s.at[0], mx_r.at[0])
    for part in range(3):
        got((wm_s, part, 4))
    got((mx_s, 0))
    mxv = mx.reshape(64, 128)
    lhs = jnp.concatenate([mxv[pl.ds(4 * core + i, 8, stride=8), :] for i in range(4)], axis=1).astype(BF16)
    mo = dot_nt(lhs, wm.reshape(2048, 512)[...])
    mos[0] = mo[:4]
    mos[1] = mo[4:]
    remote(mos.at[1 - core], mor, mx_s.at[1], mx_r.at[1], partner)
    expect((mx_s, 1), mor, mx_s.at[1], mx_r.at[1])
    mo = mos[core]
    got((mx_s, 1))
    mo = (mo + mor[...]).astype(BF16).astype(F32)
    pre = ALPHA * toks + mo
    center = jnp.mean(pre, axis=1, keepdims=True)
    var = jnp.mean(jnp.square(pre - center), axis=1, keepdims=True)
    normed = ((pre - center) * lax.rsqrt(var + NORM_EPS) * g1[...] + b1[...]).astype(BF16).astype(F32)
    nblk = jnp.concatenate([normed[:, :HALF], normed[:, HALF:]], axis=0)
    nb[own] = nblk.astype(BF16)

    for part in range(3):
        plane_send(nb, part, nb_s, nb_r)
    for i in range(3, 6):
        got((pw_s, 4 + i))
    turn(1 - core)
    for g in (0, 1, 3, 2):
        for part in range(3):
            line_send(nb, part, g, nb_s, nb_r)
    for part in range(3):
        got((nb_s, part, 4))

    nbv = nb.reshape(512, HALF)
    for u in range(2):
        sel = dot(sels[u], nbv[256 * u : 256 * (u + 1), :]).astype(BF16)
        xe[64 * u : 64 * (u + 1), :HALF] = sel[:64]
        xe[64 * u : 64 * (u + 1), HALF:] = sel[64:]
    xes = xe[...]
    hiddens = []
    for c in range(2):
        gate = dot(xes, egt[c])
        up = dot(xes, eut[c])
        hiddens.append((gate * sigmoid(gate) * up).astype(BF16))
    y2 = dot_nt(nbv[...], wd[...])
    first_half = (iota((512, 256), 0) // 4) % 2 == 0
    y = jnp.where(first_half, y2[:, :256], y2[:, 256:]).reshape(64, 8, 256)
    y = (y + pltpu.roll(y, 4, 1)).reshape(512, 256)
    yg = y[:, :128]
    weight = sigmoid(jnp.sum(yg * pick, axis=1, keepdims=True))
    branch = sigmoid(yg[:, 104:105])
    hd = yg * sigmoid(yg) * y[:, 128:] * branch
    top = (iota((512, 128), 0) // 4) % 2 == 0
    hdd = jnp.concatenate([jnp.where(top, hd, 0.0), jnp.where(top, 0.0, hd)], axis=1).astype(BF16)
    slots = (dot(hiddens[0], ed[0]) + dot(hiddens[1], ed[1])).astype(BF16)
    obv = ob.reshape(512, HALF)
    for u in range(2):
        ru = slice(256 * u, 256 * (u + 1))
        rows_u = jnp.concatenate([slots[64 * u : 64 * (u + 1), :HALF], slots[64 * u : 64 * (u + 1), HALF:]], axis=0)
        total = weight[ru] * dot(spreads[u], rows_u) + dot(hdd[ru], wdd[...])
        obv[ru, :] = total.astype(BF16)

    r1s, r2s, t1s = (r1a, r1b, r1c), (r2a, r2b, r2c), (t1a, t1b, t1c)
    spots = ((2, 0), (1, 1), (3, 2), (0, 3))
    for g, slot in spots:
        for part in range(3):
            d1, d2, _ = ORDERS[part]
            for k in (2, 1, 3):
                idx = region(part, {d1: (at[d1] + k) % 4, d2: (at[d2] + g) % 4})
                remote(
                    ob.at[idx + TAILS[part]], r1s[part].at[slot, k - 1], rs_s.at[part, slot], rs_r.at[part, slot],
                    peer({d1: k}),
                )
            expect((rs_s, part, slot), r1s[part].at[slot], rs_s.at[part, slot], rs_r.at[part, slot])
    for g, slot in spots:
        for part in range(3):
            d1, d2, d3 = ORDERS[part]
            got((rs_s, part, slot))
            idx = region(part, {d1: at[d1], d2: (at[d2] + g) % 4})
            total = ob[idx + TAILS[part]].astype(F32)
            for k in range(3):
                total = total + r1s[part][slot, k].astype(F32)
            t1s[part][slot] = total.astype(BF16)
            for k in (2, 1, 3, 0):
                if k or g:
                    remote(
                        t1s[part].at[slot, (at[d3] + k) % 4], r2s[part].at[4 * g + k - 1], rs_s.at[part, 4],
                        rs_r.at[part, 4], peer({d2: g, d3: k}),
                    )
    chans = []
    for part in range(3):
        d3 = ORDERS[part][2]
        take(r2s[part], rs_r.at[part, 4])
        total = t1s[part][3, at[d3]].astype(F32)
        for k in range(15):
            total = total + r2s[part][k].astype(F32)
        chans.append(total)
        sent[f"r{part}"] = functools.partial(take, r2s[part], rs_s.at[part, 4])
    z = ALPHA * nblk + jnp.concatenate(chans, axis=1)

    def both(v):
        v = jnp.broadcast_to(v, (8, 128))
        return (v + pltpu.roll(v, 4, 0))[:, 0:1]

    def by_half(ref):
        v = ref[...]
        return jnp.concatenate(
            [jnp.broadcast_to(v[:, :HALF], (4, HALF)), jnp.broadcast_to(v[:, HALF:], (4, HALF))], axis=0
        )

    center = both(jnp.sum(z, axis=1, keepdims=True)) * (1.0 / 2048)
    dev = z - center
    var = both(jnp.sum(dev * dev, axis=1, keepdims=True)) * (1.0 / 2048)
    res = dev * lax.rsqrt(var + NORM_EPS) * by_half(g2) + by_half(b2)
    outv[:, :HALF] = res[:4].astype(BF16)
    outv[:, HALF:] = res[4:].astype(BF16)
    c_out.append(local(outv, out_h, loc.at[0]))

    for c in c_out:
        c.wait()
    for wait in sent.values():
        wait()


def closing(a_h, s_h, out_h, nst_h, av, sv, into, out):
    ins = [pltpu.make_async_copy(s_h.at[t], sv.at[t], into.at[t]) for t in range(4)]
    ins.append(pltpu.make_async_copy(a_h, av, into.at[4]))
    outs = [pltpu.make_async_copy(sv.at[t], nst_h.at[t], out.at[t]) for t in range(4)]
    outs.append(pltpu.make_async_copy(av, out_h, out.at[4]))
    for cp in ins:
        cp.start()
    for cp, back in zip(ins, outs):
        cp.wait()
        back.start()
    for back in outs:
        back.wait()


def per_device(
    tokens, recurrent_state, query_weight, forget_weight, input_weight, outgate_weight, lower_bound, head_gain,
    mixout_weight, first_gain, first_bias, router_weight, branch_vector, dense_gate_weight, dense_up_weight,
    dense_down_weight, expert_gate_weight, expert_up_weight, expert_down_weight, second_gain, second_bias, routes,
):
    args = (
        tokens, recurrent_state, query_weight.T, forget_weight.T, input_weight.T, outgate_weight.T,
        lower_bound.reshape(8, 128), head_gain.reshape(1, 128), mixout_weight.T, first_gain.reshape(1, 2048),
        first_bias.reshape(1, 2048), router_weight.T, branch_vector.reshape(16, 128), dense_gate_weight.T,
        dense_up_weight.T, dense_down_weight, expert_gate_weight.T, expert_up_weight.T, expert_down_weight,
        second_gain.reshape(1, 2048), second_bias.reshape(1, 2048), routes.T,
    )
    lanes = [p.stop - p.start for p in LANES]
    V = pltpu.VMEM
    sem = pltpu.SemaphoreType.DMA
    scratch = [
        V((4, 2048), BF16), V((4, 2048), BF16), V((4, 8, 128, 128), F32), V((4, 8, 128, 128), F32), V((4, 2, 8, 2048), BF16),
        V((8, 128), F32), V((1, 128), F32), V((4, 4, 4, 2, 16, 512), BF16), V((1, 2048), F32), V((1, 2048), F32),
        V((8, 2048), BF16), V((16, 128), BF16), V((2, 44, 2048), BF16), V((2, 44, 2048), BF16),
        V((2, 44, 2048), BF16), V((2, 448, 2048), BF16), V((2, 448, 2048), BF16), V((2, 448, 2048), BF16),
        V((1, 2048), F32), V((1, 2048), F32), V((2, 512), jnp.int32),
        V((4, 4, 4, 8, HALF), BF16), V((4, 4, 4, 8, HALF), BF16), V((64, 8, 128), BF16), V((64, 8, 128), BF16),
        V((4, 4, 4, 8, HALF), BF16), V((128, 2048), BF16), V((512, HALF), BF16), V((256, HALF), BF16),
        V((32, 128), F32),
        *[V((4, 3, 4, 8, n), BF16) for n in lanes], *[V((15, 8, n), BF16) for n in lanes],
        *[V((4, 4, 8, n), BF16) for n in lanes],
        V((2, 32, 128), F32), V((2, 4, 2048), F32), V((4, 2048), F32), V((2, 2048, 448), BF16), V((2, 2048, 448), BF16),
        sem((21,)), sem((4,)), sem((4,)), sem((10,)), sem((10,)), sem((3, 5)), sem((3, 5)), sem(()), sem(()),
        sem((2,)), sem((2,)), sem((3, 5)), sem((3, 5)), sem((3, 5)), sem((3, 5)), sem(()), sem(()), sem((3, 5)), sem((3, 5)),
    ]
    hbm = pl.BlockSpec(memory_space=pltpu.HBM)
    free = pl.BlockSpec(memory_space=pl.ANY)
    shapes = (jax.ShapeDtypeStruct((4, 2048), BF16), jax.ShapeDtypeStruct((4, 8, 128, 128), F32))
    res = pl.pallas_call(
        kernel,
        out_shape=shapes,
        in_specs=[hbm] * 22,
        out_specs=(free, free),
        scratch_shapes=scratch,
        compiler_params=pltpu.CompilerParams(
            collective_id=0, has_side_effects=True, vmem_limit_bytes=60 * 1024 * 1024
        ),
        name="layer",
    )(*args)
    return pl.pallas_call(
        closing,
        out_shape=shapes,
        in_specs=[free] * 2,
        out_specs=(free, free),
        scratch_shapes=[V((4, 2048), BF16), V((4, 8, 128, 128), F32), sem((5,)), sem((5,))],
        compiler_params=pltpu.CompilerParams(vmem_limit_bytes=60 * 1024 * 1024),
        name="closing",
    )(*res)


def solution(mesh):
    ep = "ep"
    cols, rows = P(None, ep), P(ep, None)
    return jax.shard_map(
        per_device,
        mesh=mesh,
        in_specs=(
            rows, P(ep, None, None, None), cols, cols, cols, cols, P(), P(), cols, P(), P(), P(), P(),
            cols, cols, rows, cols, cols, rows, P(), P(), P(),
        ),
        out_specs=(rows, P(ep, None, None, None)),
        check_vma=False,
    )
```
